32 devices in a mesh: grp: 2 (over x), ep: 8 (over z, y), tp: 2 (over core).
Axes of the slice: x: 2, y: 2, z: 4, core: 2. Of those that a mesh axis runs over, the one named last changes fastest.
Arguments:
- hidden_in: bfloat16 [256, 2048], P(('grp', 'ep', 'tp')), parts along dimension 0, may hold values from -6 to 6
- query_nope: bfloat16 [256, 16, 64], P(('grp', 'ep', 'tp')), parts along dimension 0, may hold values from -102 to 102
- query_rope: bfloat16 [256, 16, 32], P(('grp', 'ep', 'tp')), parts along dimension 0, may hold values from -6 to 6
- new_latent: bfloat16 [256, 256], P(('grp', 'ep', 'tp')), parts along dimension 0, may hold values from -6 to 6
- new_rope: bfloat16 [256, 32], P(('grp', 'ep', 'tp')), parts along dimension 0, may hold values from -6 to 6
- cache_latent: bfloat16 [256, 1024, 256], P(('grp', 'ep', 'tp')), parts along dimension 0, may hold values from -6 to 6
- cache_rope: bfloat16 [256, 1024, 32], P(('grp', 'ep', 'tp')), parts along dimension 0, may hold values from -6 to 6
- lengths: int32 [256], P(('grp', 'ep', 'tp')), parts along dimension 0, may hold values from 1 to 1024, as said below
- absorb_key: bfloat16 [256, 16, 64], replicated, may hold values from -0.75 to 0.75
- value_up: bfloat16 [256, 16, 128], replicated, may hold values from -0.375 to 0.375
- out_proj: bfloat16 [2048, 2048], P(None, ('ep', 'tp')), may hold values from -0.125 to 0.125
- gain_mix: bfloat16 [2048], replicated, may hold values from 0.099609375 to 1.8984375
- gain_ffn_in: bfloat16 [2048], replicated, may hold values from 0.099609375 to 1.8984375
- router: bfloat16 [2048, 16], replicated, may hold values from -0.125 to 0.125
- routes: int32 [256, 6], P(('grp', 'ep')), parts along dimension 0, may hold values from 0 to 15, all different within a row; in each aligned block of 16 rows (0 to 15, 16 to 31, ...) at most 12 rows name the same one
- expert_gate: bfloat16 [16, 2048, 256], P(('ep', 'tp')), may hold values from -0.125 to 0.125
- expert_up: bfloat16 [16, 2048, 256], P(('ep', 'tp')), may hold values from -0.125 to 0.125
- expert_down: bfloat16 [16, 256, 2048], P(('ep', 'tp')), may hold values from -0.375 to 0.375
- shared_gate: bfloat16 [2048, 256], replicated, may hold values from -0.125 to 0.125
- shared_up: bfloat16 [2048, 256], replicated, may hold values from -0.125 to 0.125
- shared_down: bfloat16 [256, 2048], replicated, may hold values from -0.375 to 0.375
- gain_ffn_out: bfloat16 [2048], replicated, may hold values from 0.099609375 to 1.8984375
Outputs:
- layer_out: bfloat16 [256, 2048], P(('grp', 'ep', 'tp')), parts along dimension 0
The draws below stay inside these ranges and needn't reach their ends.
There are 2 independent parts, one for each index of `grp`. The reference program is written for one: setup_inputs(seed, part) draws one part's arguments, and reference() takes and returns one part's arrays. A program takes and returns all parts, laid end to end along the dimension named above; an argument that names none is the same for every part. Nothing has to cross between parts.
Inputs may be any that keep to these rules, and one draw needn't show every extreme that they name: `lengths`: every sequence holds 1 to 1024 cached positions, and some sequence holds 1024. `routes`: each row names 6 different experts; in each aligned block of 16 rows (the rows of one index of ep) no expert is named by more than 12 rows, and in some block some expert is named by exactly 12 rows.
All inputs are finite; a program needn't handle non-finite values.
Results may differ from the reference program's by a relative error of at most 0.015.
Values may be sent and summed in bfloat16 or wider, within the bound.
A program may use at most 64 MiB of HBM per device.

```python
import math
import jax
import jax.numpy as jnp
import numpy as np
from jax import lax

D = 2048
HEADS = 16
NOPE = 64
ROPE = 32
VHEAD = 128
LAT = 256
FE = 256
FS = 256
TOPK = 6
CTX = 1024
SEQ_DEV = 8
NSEQ = 128
TOK_GROUP = 16
EXPERTS = 16
CAP = 12
N_EP = 8


def draw_query_nope(key, part):
    base_key = jax.random.fold_in(jax.random.fold_in(key, 23), 0)
    values = jnp.clip(jax.random.normal(base_key, (NSEQ, HEADS, NOPE), jnp.float32), -6.0, 6.0)
    return values.astype(jnp.bfloat16)


def draw_lengths(key, part):
    level_key, value_key, pick_key = jax.random.split(jax.random.fold_in(key, 11), 3)
    device_count = NSEQ // SEQ_DEV
    level_draw = jax.random.randint(level_key, (device_count,), 1, 5)
    length_limit = jnp.maximum(jnp.repeat(level_draw * level_draw * CTX // 16, SEQ_DEV), 1)
    raw_draw = jax.random.randint(value_key, (NSEQ,), 0, 1 << 20)
    drawn_lengths = 1 + raw_draw % length_limit
    chosen_row = jax.random.randint(pick_key, (), 0, NSEQ)
    drawn_lengths = jnp.where(jnp.arange(NSEQ) == chosen_row, CTX, drawn_lengths)
    return drawn_lengths.astype(jnp.int32)


def steps_of(stream_key, shape, pieces, low, high):
    def one(axis_at, shards_of):
        draws = jax.random.uniform(jax.random.fold_in(jax.random.fold_in(stream_key, 6), axis_at), (shards_of,), jnp.float32, low / len(pieces), high / len(pieces))
        return jnp.repeat(jnp.exp(draws), shape[axis_at] // shards_of).reshape((-1,) + (1,) * (len(shape) - axis_at - 1))

    gain = one(*pieces[0])
    for cut in pieces[1:]:
        gain = gain * one(*cut)
    return gain


def routed_block(own_key, own, number, rows, count, top, limit, slope):
    order = jax.random.permutation(own_key, count)
    crowded, usual = shares(count, rows * top, limit, slope, True), shares(count, rows * top, limit, slope, False)
    places = jnp.arange(count)

    def named(sizes, offset_by):
        used = int((sizes > 0).sum())
        fixed = max(1, used // 4)
        shifted = fixed + (places - fixed + offset_by * (used - fixed)) % max(1, count - fixed)
        return jnp.zeros((count,), jnp.int32).at[order[jnp.where(places < fixed, places, shifted)]].set(jnp.asarray(sizes, jnp.int32))

    sizes = jnp.where(number % 4 == 0, named(crowded, number // 4), named(usual, number - number // 4 - 1))
    mixed = jax.random.permutation(jax.random.fold_in(own, 3), count)
    giver, sink = mixed[0:count // 2 * 2:2], mixed[1:count // 2 * 2:2]
    margin = jnp.minimum(sizes[giver] - 1, limit - sizes[sink]) // 2
    margin = jnp.where((giver == order[0]) | (sink == order[0]) | (sizes[sink] == 0), 0, jnp.maximum(margin, 0))
    shifted = jax.random.randint(jax.random.fold_in(own, 4), (count // 2,), 0, 1 << 20) % (margin + 1)
    sizes = sizes.at[giver].add(-shifted).at[sink].add(shifted)
    items = jnp.searchsorted(jnp.cumsum(sizes), jnp.arange(rows * top), side="right").astype(jnp.int32)
    grid = items.reshape(top, rows).T
    grid = grid[jax.random.permutation(jax.random.fold_in(own, 1), rows)]
    offset_by = jax.random.randint(jax.random.fold_in(own, 2), (rows, 1), 0, top)
    return jnp.take_along_axis(grid, (jnp.arange(top)[None, :] + offset_by) % top, axis=1)


def shares(count, total, limit, lean, full):
    loads = [(1 << 20) // math.isqrt(rank ** lean) + 1 for rank in range(1, count + 1)]
    largest = limit if full else min(limit, max(-(-total // count), total * loads[0] // sum(loads)))
    least = 1 if total - largest >= count - 1 else 0
    counts, surplus = [largest] + [least] * (count - 1), total - largest - least * (count - 1)
    while surplus > 0:
        candidates = [i for i in range(1, count) if counts[i] < largest] or [i for i in range(1, count) if counts[i] < limit]
        whole, budget = sum([loads[i] for i in candidates]), surplus
        for i in candidates:
            addition = min(limit - counts[i], max(1, budget * loads[i] // whole), surplus)
            counts[i] = counts[i] + addition
            surplus = surplus - addition
    return np.array(counts)


def bell_draw(rng, shape, width, reach, pieces=(), kind=jnp.bfloat16):
    drawn = jax.random.normal(rng, shape, jnp.float32) * width
    if len(pieces) > 0:
        drawn = steps_of(rng, shape, pieces, -0.22, 0.18) * drawn
    return jnp.clip(drawn, min=-reach, max=reach).astype(kind)


def setup_inputs(seed: int = 0, part: int = 0) -> dict:
    key_of = jax.random.split(jax.random.key(seed), 23)
    own_keys = jax.random.split(jax.random.fold_in(key_of[22], part), 23)
    hidden_in = bell_draw(own_keys[0], (NSEQ, D), 1.0, 6.0, ((0, 16),))
    query_nope = draw_query_nope(jax.random.fold_in(jax.random.fold_in(key_of[22], part), 71), part)
    query_rope = bell_draw(own_keys[2], (NSEQ, HEADS, ROPE), 1.0, 6.0, ((0, 16),))
    new_latent = bell_draw(own_keys[3], (NSEQ, LAT), 1.0, 6.0, ((0, 16),))
    new_rope = bell_draw(own_keys[4], (NSEQ, ROPE), 1.0, 6.0, ((0, 16),))
    cache_latent = bell_draw(own_keys[5], (NSEQ, CTX, LAT), 1.0, 6.0, ((0, 16),))
    cache_rope = bell_draw(own_keys[6], (NSEQ, CTX, ROPE), 1.0, 6.0, ((0, 16),))
    lengths = draw_lengths(jax.random.fold_in(jax.random.fold_in(key_of[22], part), 71), part)
    absorb_key = bell_draw(key_of[8], (LAT, HEADS, NOPE), NOPE ** -0.5, 0.75)
    value_up = bell_draw(key_of[9], (LAT, HEADS, VHEAD), LAT ** -0.5, 0.375)
    out_proj = bell_draw(key_of[10], (HEADS * VHEAD, D), (HEADS * VHEAD) ** -0.5, 0.125, ((1, 16),))
    gain_mix = jnp.clip(1.0 + 0.18 * jax.random.normal(key_of[11], (D,), jnp.float32), 0.099609375, 1.8984375).astype(jnp.bfloat16)
    gain_ffn_in = jnp.clip(1.0 + 0.18 * jax.random.normal(key_of[12], (D,), jnp.float32), 0.099609375, 1.8984375).astype(jnp.bfloat16)
    router = bell_draw(key_of[13], (D, EXPERTS), D ** -0.5, 0.125)
    routes_keys = jax.random.split(jax.random.fold_in(own_keys[14], 1), NSEQ // TOK_GROUP)
    routes_turns = jax.random.permutation(jax.random.fold_in(own_keys[14], 3), NSEQ // TOK_GROUP)
    routes = jax.vmap(lambda own, number: routed_block(jax.random.fold_in(own_keys[14], 2), own, number, TOK_GROUP, EXPERTS, TOPK, CAP, 2))(routes_keys, routes_turns).reshape((NSEQ, TOPK))
    expert_gate = bell_draw(key_of[15], (EXPERTS, D, FE), D ** -0.5, 0.125, ((0, 16),))
    expert_up = bell_draw(key_of[16], (EXPERTS, D, FE), D ** -0.5, 0.125, ((0, 16),))
    expert_down = bell_draw(key_of[17], (EXPERTS, FE, D), FE ** -0.5, 0.375, ((0, 16),))
    shared_gate = bell_draw(key_of[18], (D, FS), D ** -0.5, 0.125)
    shared_up = bell_draw(key_of[19], (D, FS), D ** -0.5, 0.125)
    shared_down = bell_draw(key_of[20], (FS, D), FS ** -0.5, 0.375)
    gain_ffn_out = jnp.clip(1.0 + 0.18 * jax.random.normal(key_of[21], (D,), jnp.float32), 0.099609375, 1.8984375).astype(jnp.bfloat16)
    return dict(hidden_in=hidden_in, query_nope=query_nope, query_rope=query_rope, new_latent=new_latent, new_rope=new_rope, cache_latent=cache_latent, cache_rope=cache_rope, lengths=lengths, absorb_key=absorb_key, value_up=value_up, out_proj=out_proj, gain_mix=gain_mix, gain_ffn_in=gain_ffn_in, router=router, routes=routes, expert_gate=expert_gate, expert_up=expert_up, expert_down=expert_down, shared_gate=shared_gate, shared_up=shared_up, shared_down=shared_down, gain_ffn_out=gain_ffn_out)


rope_theta = 10000.0
norm_eps = 1e-06
routed_scale = 2.5
masked_score = -1e+30

def normalize(values):
    return values * lax.rsqrt(lax.optimization_barrier(jnp.mean(values * values, axis=-1, keepdims=True)) + norm_eps)

def rotate(values, positions):
    half_dim = values.shape[-1] // 2
    inverse = rope_theta ** (-jnp.arange(half_dim, dtype=jnp.float32) * 2.0 / values.shape[-1])
    angles = positions * inverse
    cosine = jnp.cos(angles)
    sine_table = jnp.sin(angles)
    first_half = values[..., :half_dim]
    second_half = values[..., half_dim:]
    return jnp.concatenate([first_half * cosine - second_half * sine_table, first_half * sine_table + second_half * cosine], axis=-1)

def swiglu(flat_rows, gate_w, up_w, down_w):
    gate_part = jnp.dot(flat_rows, gate_w, preferred_element_type=jnp.float32)
    up_part = jnp.dot(flat_rows, up_w, preferred_element_type=jnp.float32)
    inner_rows = (jax.nn.silu(gate_part) * up_part).astype(jnp.bfloat16)
    return jnp.dot(inner_rows, down_w, preferred_element_type=jnp.float32).astype(jnp.bfloat16)

def attend_group(group_args):
    query_latent, query_pe, latent_block, rope_block, latent_new, key_new, group_lengths = group_args
    score_scale = (NOPE + ROPE) ** (-0.5)
    cache_scores = (jnp.einsum('shc,skc->shk', query_latent.astype(jnp.float32), latent_block.astype(jnp.float32)) + jnp.einsum('shr,skr->shk', query_pe.astype(jnp.float32), rope_block.astype(jnp.float32))) * score_scale
    new_score = (jnp.einsum('shc,sc->sh', query_latent.astype(jnp.float32), latent_new.astype(jnp.float32)) + jnp.einsum('shr,sr->sh', query_pe.astype(jnp.float32), key_new.astype(jnp.float32))) * score_scale
    in_range = jnp.arange(CTX, dtype=jnp.int32)[None, None, :] < group_lengths[:, None, None]
    cache_scores = jnp.where(in_range, cache_scores, masked_score)
    row_max = jnp.maximum(lax.optimization_barrier(jnp.max(cache_scores, axis=-1)), new_score)
    cache_exp = jnp.exp(cache_scores - row_max[..., None])
    new_exp = jnp.exp(new_score - row_max)
    weight_total = lax.optimization_barrier(jnp.sum(cache_exp, axis=-1)) + new_exp
    cache_weights = lax.optimization_barrier(cache_exp.astype(jnp.bfloat16)).astype(jnp.float32)
    new_weight = lax.optimization_barrier(new_exp.astype(jnp.bfloat16)).astype(jnp.float32)
    weighted = jnp.einsum('shk,skc->shc', cache_weights, latent_block.astype(jnp.float32)) + new_weight[..., None] * latent_new.astype(jnp.float32)[:, None, :]
    return (weighted / weight_total[..., None]).astype(jnp.bfloat16)

def expert_apply(expert_args):
    flat_rows, gate_w, up_w, down_w = expert_args
    return swiglu(flat_rows, gate_w, up_w, down_w)

def reference(hidden_in, query_nope, query_rope, new_latent, new_rope, cache_latent, cache_rope, lengths, absorb_key, value_up, out_proj, gain_mix, gain_ffn_in, router, routes, expert_gate, expert_up, expert_down, shared_gate, shared_up, shared_down, gain_ffn_out):
    seq_count = hidden_in.shape[0]
    group_count = seq_count // SEQ_DEV
    positions = lengths.astype(jnp.float32)
    query_latent = jnp.einsum('shn,chn->shc', query_nope.astype(jnp.float32), absorb_key.astype(jnp.float32)).astype(jnp.bfloat16)
    query_pe = rotate(query_rope.astype(jnp.float32), positions[:, None, None]).astype(jnp.bfloat16)
    latent_new = normalize(new_latent.astype(jnp.float32)).astype(jnp.bfloat16)
    key_new = rotate(new_rope.astype(jnp.float32), positions[:, None]).astype(jnp.bfloat16)

    def grouped(values):
        return values.reshape((group_count, SEQ_DEV) + values.shape[1:])
    latent_out = lax.map(attend_group, (grouped(query_latent), grouped(query_pe), grouped(cache_latent), grouped(cache_rope), grouped(latent_new), grouped(key_new), grouped(lengths)))
    latent_out = latent_out.reshape(seq_count, HEADS, LAT)
    heads_out = jnp.einsum('shc,chv->shv', latent_out.astype(jnp.float32), value_up.astype(jnp.float32)).astype(jnp.bfloat16).reshape(seq_count, HEADS * VHEAD)
    mixed_rows = jnp.dot(heads_out, out_proj, preferred_element_type=jnp.float32).astype(jnp.bfloat16)
    after_mix = (hidden_in.astype(jnp.float32) + gain_mix.astype(jnp.float32) * normalize(mixed_rows.astype(jnp.float32))).astype(jnp.bfloat16)
    ffn_in = (normalize(after_mix.astype(jnp.float32)) * gain_ffn_in.astype(jnp.float32)).astype(jnp.bfloat16)
    affinity = jax.nn.sigmoid(jnp.dot(ffn_in, router, preferred_element_type=jnp.float32))
    chosen = jnp.take_along_axis(affinity, routes, axis=1)
    route_weights = chosen / lax.optimization_barrier(jnp.sum(chosen, axis=-1, keepdims=True)) * routed_scale
    pair_count = TOK_GROUP * TOPK
    expert_ids = routes.reshape(N_EP, pair_count)
    order_index = jnp.arange(pair_count, dtype=jnp.int32)
    same_expert = expert_ids[:, :, None] == expert_ids[:, None, :]
    earlier = order_index[None, :] < order_index[:, None]
    slot_number = lax.optimization_barrier(jnp.sum(jnp.logical_and(same_expert, earlier[None]), axis=2)).astype(jnp.int32)
    slot_number = slot_number.reshape(seq_count, TOPK)
    group_index = (jnp.arange(seq_count, dtype=jnp.int32) // TOK_GROUP)[:, None]
    slot_index = (routes * (N_EP * CAP) + group_index * CAP + slot_number).astype(jnp.int32)
    buffer = jnp.zeros((EXPERTS * N_EP * CAP, D), jnp.bfloat16)
    buffer = buffer.at[slot_index.reshape(-1)].set(jnp.repeat(ffn_in, TOPK, axis=0))
    outputs = lax.map(expert_apply, (buffer.reshape(EXPERTS, N_EP * CAP, D), expert_gate, expert_up, expert_down))
    picked = outputs.reshape(EXPERTS * N_EP * CAP, D)[slot_index]
    routed = lax.optimization_barrier(jnp.sum(picked.astype(jnp.float32) * route_weights[..., None], axis=1))
    shared = swiglu(ffn_in, shared_gate, shared_up, shared_down)
    combined = routed + shared.astype(jnp.float32)
    return (after_mix.astype(jnp.float32) + gain_ffn_out.astype(jnp.float32) * normalize(combined)).astype(jnp.bfloat16)
```

```python
import functools

import jax
import jax.numpy as jnp
from jax import lax
from jax.experimental import pallas as pl
from jax.experimental.pallas import tpu as pltpu
from jax.sharding import PartitionSpec as P

ABLK = 512


rope_theta = 10000.0
norm_eps = 1e-06
routed_scale = 2.5
masked_score = -1e30


def normalize(values):
    return values * lax.rsqrt(jnp.mean(values * values, axis=-1, keepdims=True) + norm_eps)


def rotate(values, positions):
    half_dim = values.shape[-1] // 2
    inverse = rope_theta ** (-jnp.arange(half_dim, dtype=jnp.float32) * 2.0 / values.shape[-1])
    angles = positions * inverse
    cosine = jnp.cos(angles)
    sine_table = jnp.sin(angles)
    first_half = values[..., :half_dim]
    second_half = values[..., half_dim:]
    return jnp.concatenate(
        [
            first_half * cosine - second_half * sine_table,
            first_half * sine_table + second_half * cosine,
        ],
        axis=-1,
    )


def swiglu(flat_rows, gate_w, up_w, down_w):
    gate_part = jnp.dot(flat_rows, gate_w, preferred_element_type=jnp.float32)
    up_part = jnp.dot(flat_rows, up_w, preferred_element_type=jnp.float32)
    inner_rows = (jax.nn.silu(gate_part) * up_part).astype(jnp.bfloat16)
    return jnp.dot(inner_rows, down_w, preferred_element_type=jnp.float32).astype(jnp.bfloat16)


def local_wide(
    hidden_in,
    query_nope,
    query_rope,
    new_latent,
    new_rope,
    cache_latent,
    cache_rope,
    lengths,
    absorb_key,
    value_up,
    out_proj,
    gain_mix,
    gain_ffn_in,
    router,
    routes,
    expert_gate,
    expert_up,
    expert_down,
    shared_gate,
    shared_up,
    shared_down,
    gain_ffn_out,
):
    seq_count = hidden_in.shape[0]
    positions = lengths.astype(jnp.float32)
    query_latent = jnp.einsum(
        "shn,chn->shc", query_nope, absorb_key, preferred_element_type=jnp.float32
    ).astype(jnp.bfloat16)
    query_pe = rotate(query_rope.astype(jnp.float32), positions[:, None, None]).astype(jnp.bfloat16)
    latent_new = normalize(new_latent.astype(jnp.float32)).astype(jnp.bfloat16)
    key_new = rotate(new_rope.astype(jnp.float32), positions[:, None]).astype(jnp.bfloat16)
    score_scale = (query_nope.shape[-1] + query_rope.shape[-1]) ** (-0.5)
    new_score = (
        jnp.einsum("shc,sc->sh", query_latent, latent_new, preferred_element_type=jnp.float32)
        + jnp.einsum("shr,sr->sh", query_pe, key_new, preferred_element_type=jnp.float32)
    ) * score_scale

    def attend_block(block_index, loop_state):
        running_max, weight_total, weighted_sum = loop_state
        block_start = block_index * ABLK
        block_latent = lax.dynamic_slice_in_dim(cache_latent, block_start, ABLK, 1)
        block_rope = lax.dynamic_slice_in_dim(cache_rope, block_start, ABLK, 1)
        scores = (
            jnp.einsum(
                "shc,skc->shk", query_latent, block_latent, preferred_element_type=jnp.float32
            )
            + jnp.einsum("shr,skr->shk", query_pe, block_rope, preferred_element_type=jnp.float32)
        ) * score_scale
        key_index = block_start + lax.iota(jnp.int32, ABLK)
        in_range = key_index[None, None, :] < lengths[:, None, None]
        scores = jnp.where(in_range, scores, masked_score)
        new_max = jnp.maximum(running_max, jnp.max(scores, axis=-1))
        rescale = jnp.exp(running_max - new_max)
        weights = jnp.exp(scores - new_max[..., None])
        weight_total = weight_total * rescale + jnp.sum(weights, axis=-1)
        weighted_sum = weighted_sum * rescale[..., None] + jnp.einsum(
            "shk,skc->shc",
            weights.astype(jnp.bfloat16),
            block_latent,
            preferred_element_type=jnp.float32,
        )
        return (new_max, weight_total, weighted_sum)

    longest = jnp.max(lengths)
    block_count = (longest + ABLK - 1) // ABLK
    ones_start = jnp.ones_like(new_score)
    sum_start = ones_start[..., None] * latent_new.astype(jnp.float32)[:, None, :]
    final_max, weight_total, weighted_sum = lax.fori_loop(
        0, block_count, attend_block, (new_score, ones_start, sum_start)
    )
    latent_out = (weighted_sum / weight_total[..., None]).astype(jnp.bfloat16)
    heads_out = (
        jnp.einsum("shc,chv->shv", latent_out, value_up, preferred_element_type=jnp.float32)
        .astype(jnp.bfloat16)
        .reshape(seq_count, -1)
    )
    column_rows = jnp.dot(
        lax.all_gather(heads_out, ("ep", "tp"), axis=0, tiled=True),
        out_proj,
        preferred_element_type=jnp.float32,
    ).astype(jnp.bfloat16)
    mixed_rows = lax.all_to_all(column_rows, ("ep", "tp"), split_axis=0, concat_axis=1, tiled=True)
    after_mix = (
        hidden_in.astype(jnp.float32)
        + gain_mix.astype(jnp.float32) * normalize(mixed_rows.astype(jnp.float32))
    ).astype(jnp.bfloat16)
    ffn_in = (normalize(after_mix.astype(jnp.float32)) * gain_ffn_in.astype(jnp.float32)).astype(
        jnp.bfloat16
    )
    affinity = jax.nn.sigmoid(jnp.dot(ffn_in, router, preferred_element_type=jnp.float32))
    experts_total = router.shape[1]
    own_start = lax.axis_index("tp") * seq_count
    own_routes = lax.dynamic_slice_in_dim(routes, own_start, seq_count, 0)
    choose = own_routes[..., None] == lax.iota(jnp.int32, experts_total)[None, None, :]
    chosen = jnp.sum(jnp.where(choose, affinity[:, None, :], 0.0), axis=-1)
    route_weights = chosen / jnp.sum(chosen, axis=-1, keepdims=True) * routed_scale
    group_rows, top_count = routes.shape
    capacity = 2 * ((group_rows * top_count + experts_total - 1) // experts_total)
    flat_routes = routes.reshape(-1)
    order_index = lax.iota(jnp.int32, group_rows * top_count)
    same_expert = flat_routes[:, None] == flat_routes[None, :]
    earlier = order_index[None, :] < order_index[:, None]
    slot_number = jnp.sum(jnp.logical_and(same_expert, earlier), axis=1)
    slot_number = slot_number.reshape(group_rows, top_count)
    own_slots = lax.dynamic_slice_in_dim(slot_number, own_start, seq_count, 0)
    slot_index = own_routes * capacity + own_slots
    slots_total = experts_total * capacity
    slot_table = jnp.any(
        slot_index[None, :, :] == lax.iota(jnp.int32, slots_total)[:, None, None], axis=-1
    ).astype(jnp.bfloat16)
    outgoing_terms = jnp.dot(slot_table, ffn_in, preferred_element_type=jnp.float32)
    outgoing = outgoing_terms.astype(jnp.bfloat16).reshape(experts_total, capacity, -1)
    received = lax.all_to_all(outgoing, ("ep", "tp"), split_axis=0, concat_axis=0, tiled=True)
    ep_count = lax.axis_size("ep")
    tp_count = lax.axis_size("tp")
    item_count = received.shape[1]
    width = received.shape[2]
    merged = jnp.sum(received.reshape(ep_count, tp_count, item_count, width), axis=1)
    outputs = swiglu(
        merged.reshape(ep_count * item_count, width), expert_gate[0], expert_up[0], expert_down[0]
    )
    copies = jnp.broadcast_to(
        outputs.reshape(ep_count, 1, item_count, width), (ep_count, tp_count, item_count, width)
    )
    copies = copies.reshape(ep_count * tp_count, item_count, width)
    returned = lax.all_to_all(copies, ("ep", "tp"), split_axis=0, concat_axis=0, tiled=True)
    picked = returned.reshape(slots_total, -1)[slot_index]
    routed = jnp.sum(picked.astype(jnp.float32) * route_weights[..., None], axis=1)
    shared = swiglu(ffn_in, shared_gate, shared_up, shared_down)
    combined = routed + shared.astype(jnp.float32)
    return (
        after_mix.astype(jnp.float32) + gain_ffn_out.astype(jnp.float32) * normalize(combined)
    ).astype(jnp.bfloat16)


def fused_kernel(
    grid_p,
    grid_q,
    score_scale,
    ql_ref,
    qp_ref,
    lnew_ref,
    knew_ref,
    len_ref,
    own_ref,
    cl_hbm,
    cr_hbm,
    vup_hbm,
    wo_hbm,
    gain_ref,
    router_hbm,
    eg_hbm,
    eu_hbm,
    ed_hbm,
    sg_hbm,
    su_hbm,
    sd_hbm,
    out_ref,
    cl,
    cr,
    vup,
    wo,
    router,
    eg,
    eu,
    ed,
    sg,
    su,
    sd,
    xbuf,
    hbuf,
    cbuf,
    lat,
    norm_rows,
    mix_rows,
    terms,
    sib,
    part,
    back,
    cache_sem,
    rope_sem,
    weight_sem,
    ag_send,
    ag_recv,
    sib_send,
    sib_recv,
    back_send,
    back_recv,
):
    seq_count, heads, latent = ql_ref.shape
    width = out_ref.shape[1]
    ep_count = grid_p * grid_q
    device_count = 2 * ep_count
    total_rows = device_count * seq_count
    me_e = lax.axis_index("ep")
    me_t = lax.axis_index("tp")
    other_t = 1 - me_t
    p = me_e // grid_q
    q = me_e % grid_q
    me = me_e * 2 + me_t

    def device(e, t):
        return {"ep": e, "tp": t}

    sibling = device(me_e, other_t)
    barrier = pltpu.get_barrier_semaphore()
    for step in range(1, ep_count):
        pl.semaphore_signal(
            barrier,
            inc=1,
            device_id=device((me_e + step) % ep_count, me_t),
            device_id_type=pl.DeviceIdType.MESH,
        )
    pl.semaphore_signal(
        barrier, inc=1, device_id=sibling, device_id_type=pl.DeviceIdType.MESH
    )

    cache_copies = []
    for s in range(seq_count):
        pair = (
            pltpu.make_async_copy(cl_hbm.at[s], cl.at[s], cache_sem.at[s]),
            pltpu.make_async_copy(cr_hbm.at[s], cr.at[s], rope_sem.at[s]),
        )
        pair[0].start()
        pair[1].start()
        cache_copies.append(pair)
    weight_copies = []
    moves = (
        (vup_hbm, vup),
        (wo_hbm, wo),
        (router_hbm, router),
        (eg_hbm, eg),
        (eu_hbm, eu),
        (ed_hbm, ed),
        (sg_hbm, sg),
        (su_hbm, su),
        (sd_hbm, sd),
    )
    for index, (source, target) in enumerate(moves):
        copy = pltpu.make_async_copy(source, target, weight_sem.at[index])
        copy.start()
        weight_copies.append(copy)
    xbuf[me] = own_ref[...]

    line_steps = list(range(1, grid_p))
    pending = []

    class Gather:
        def __init__(self, buf, which):
            self.buf, self.which, self.count = buf, which, 0

        def send(self, slot, target):
            copy = pltpu.make_async_remote_copy(
                src_ref=self.buf.at[slot],
                dst_ref=self.buf.at[slot],
                send_sem=ag_send.at[self.which, self.count],
                recv_sem=ag_recv.at[self.which, slot],
                device_id=target,
                device_id_type=pl.DeviceIdType.MESH,
            )
            copy.start()
            pending.append(copy)
            self.count += 1

        def arrive(self, slot):
            pltpu.make_async_remote_copy(
                src_ref=self.buf.at[slot],
                dst_ref=self.buf.at[slot],
                send_sem=ag_send.at[self.which, 0],
                recv_sem=ag_recv.at[self.which, slot],
                device_id=sibling,
                device_id_type=pl.DeviceIdType.MESH,
            ).wait_recv()

        def line(self, step):
            return (p + step) % grid_p

        def first(self):
            for step in sorted(line_steps, key=lambda v: -min(v, grid_p - v)):
                self.send(me, device(self.line(step) * grid_q + q, me_t))
            for turn in range(1, grid_q):
                self.send(me, device(p * grid_q + (q + turn) % grid_q, me_t))
            self.send(me, sibling)

        def second(self):
            for step in sorted(line_steps, key=lambda v: min(v, grid_p - v)):
                slot = (self.line(step) * grid_q + q) * 2 + me_t
                self.arrive(slot)
                for turn in range(1, grid_q):
                    self.send(slot, device(p * grid_q + (q + turn) % grid_q, me_t))
                self.send(slot, sibling)

        def third(self):
            for step in sorted([0] + line_steps, key=lambda v: min(v, grid_p - v)):
                for turn in range(1, grid_q):
                    slot = (self.line(step) * grid_q + (q + turn) % grid_q) * 2 + me_t
                    self.arrive(slot)
                    self.send(slot, sibling)

        def last(self):
            for e in range(ep_count):
                self.arrive(e * 2 + other_t)

    context = cl.shape[1]
    key_index = lax.broadcasted_iota(jnp.int32, (heads, context), 1)

    def attend(s):
        cache_copies[s][0].wait()
        cache_copies[s][1].wait()
        q_lat = ql_ref[s]
        q_pe = qp_ref[s]
        keys = cl[s]
        dims = (((1,), (1,)), ((), ()))
        scores = (
            lax.dot_general(q_lat, keys, dims, preferred_element_type=jnp.float32)
            + lax.dot_general(q_pe, cr[s], dims, preferred_element_type=jnp.float32)
        ) * score_scale
        new_row = lnew_ref[s : s + 1, :].astype(jnp.float32)
        key_row = knew_ref[s : s + 1, :].astype(jnp.float32)
        new_score = (
            jnp.sum(q_lat.astype(jnp.float32) * new_row, axis=-1, keepdims=True)
            + jnp.sum(q_pe.astype(jnp.float32) * key_row, axis=-1, keepdims=True)
        ) * score_scale
        scores = jnp.where(key_index < len_ref[s], scores, masked_score)
        row_max = jnp.maximum(jnp.max(scores, axis=-1, keepdims=True), new_score)
        weights = jnp.exp(scores - row_max)
        new_weight = jnp.exp(new_score - row_max)
        weight_total = jnp.sum(weights, axis=-1, keepdims=True) + new_weight
        weighted = jnp.dot(weights.astype(jnp.bfloat16), keys, preferred_element_type=jnp.float32)
        weighted = weighted + new_weight.astype(jnp.bfloat16).astype(jnp.float32) * new_row
        lat[s * heads : (s + 1) * heads, :] = (weighted / weight_total).astype(jnp.bfloat16)

    rows_gather = Gather(xbuf, 0)
    cut_a, cut_b = seq_count // 2, seq_count - seq_count // 4
    for s in range(cut_a):
        attend(s)
    pl.semaphore_wait(barrier, ep_count)
    rows_gather.first()
    for s in range(cut_a, cut_b):
        attend(s)
    rows_gather.second()
    for s in range(cut_b, seq_count):
        attend(s)

    weight_copies[0].wait()
    value_dim = width_of_head(vup, heads)
    spread = jnp.dot(lat[...], vup[...], preferred_element_type=jnp.float32)
    own_heads = []
    head_row = lax.broadcasted_iota(jnp.int32, (seq_count, heads, value_dim), 1)
    for h in range(heads):
        block = spread[:, h * value_dim : (h + 1) * value_dim].reshape(seq_count, heads, value_dim)
        own_heads.append(jnp.sum(jnp.where(head_row == h, block, 0.0), axis=1))
    hbuf[me] = jnp.concatenate(own_heads, axis=1).astype(jnp.bfloat16)
    heads_gather = Gather(hbuf, 1)
    heads_gather.first()
    rows_gather.third()
    heads_gather.second()
    heads_gather.third()
    rows_gather.last()
    weight_copies[1].wait()
    heads_gather.last()

    flat_heads = hbuf[...].reshape(total_rows, hbuf.shape[2])
    cbuf[me] = jnp.dot(flat_heads, wo[...], preferred_element_type=jnp.float32).astype(jnp.bfloat16)
    columns_gather = Gather(cbuf, 2)
    columns_gather.first()
    columns_gather.second()
    columns_gather.third()
    columns_gather.last()

    gains = gain_ref[...].astype(jnp.float32)
    mixed = jnp.concatenate([cbuf[o] for o in range(device_count)], axis=1).astype(jnp.float32)
    stage = xbuf[...].reshape(total_rows, xbuf.shape[2])
    after_mix = (stage[:, :width].astype(jnp.float32) + gains[0:1] * normalize(mixed)).astype(
        jnp.bfloat16
    )
    mix_rows[...] = after_mix.reshape(mix_rows.shape)
    ffn_in = (normalize(after_mix.astype(jnp.float32)) * gains[1:2]).astype(jnp.bfloat16)
    norm_rows[...] = ffn_in.reshape(norm_rows.shape)
    weight_copies[2].wait()
    affinity = jax.nn.sigmoid(jnp.dot(ffn_in, router[...], preferred_element_type=jnp.float32))
    hot = stage[:, width : width + affinity.shape[1]].astype(jnp.float32)
    chosen = affinity * hot
    lane = lax.broadcasted_iota(jnp.int32, chosen.shape, 1)
    mine = jnp.sum(jnp.where(lane == me, chosen, 0.0), axis=1, keepdims=True)
    mine = mine / jnp.sum(chosen, axis=1, keepdims=True) * routed_scale
    for copy in weight_copies[3:6]:
        copy.wait()
    expert_out = swiglu(ffn_in, eg[...], eu[...], ed[...])
    scaled = (expert_out.astype(jnp.float32) * mine).astype(jnp.bfloat16)
    terms[...] = scaled.reshape(terms.shape)

    def to_sibling(step):
        e = (me_e + step) % ep_count
        return pltpu.make_async_remote_copy(
            src_ref=terms.at[e * 2 + other_t],
            dst_ref=sib.at[e],
            send_sem=sib_send.at[step],
            recv_sem=sib_recv.at[e],
            device_id=sibling,
            device_id_type=pl.DeviceIdType.MESH,
        )

    order = sorted(range(1, ep_count), key=lambda v: -min(v, ep_count - v)) + [0]
    sib_copies = [to_sibling(step) for step in order]
    for copy in sib_copies:
        copy.start()
    sends = []
    for step in order:
        e = (me_e + step) % ep_count
        to_sibling(step).wait_recv()
        paired = terms[e * 2 + me_t].astype(jnp.float32) + sib[e].astype(jnp.float32)
        if step == 0:
            routed = paired
        else:
            part[e] = paired.astype(jnp.bfloat16)
            copy = pltpu.make_async_remote_copy(
                src_ref=part.at[e],
                dst_ref=back.at[me_e],
                send_sem=back_send.at[step],
                recv_sem=back_recv.at[me_e],
                device_id=device(e, me_t),
                device_id_type=pl.DeviceIdType.MESH,
            )
            copy.start()
            sends.append(copy)
    for copy in weight_copies[6:9]:
        copy.wait()
    combined = routed + swiglu(norm_rows[me], sg[...], su[...], sd[...]).astype(jnp.float32)
    for step in reversed(order[:-1]):
        e = (me_e + step) % ep_count
        pltpu.make_async_remote_copy(
            src_ref=part.at[e],
            dst_ref=back.at[e],
            send_sem=back_send.at[step],
            recv_sem=back_recv.at[e],
            device_id=device(e, me_t),
            device_id_type=pl.DeviceIdType.MESH,
        ).wait_recv()
        combined = combined + back[e].astype(jnp.float32)
    out_ref[...] = (
        mix_rows[me].astype(jnp.float32) + gains[2:3] * normalize(combined)
    ).astype(jnp.bfloat16)
    for copy in pending + sib_copies + sends:
        copy.wait_send()


def width_of_head(flat, heads):
    return flat.shape[1] // heads


def local_fused(
    hidden_in,
    query_nope,
    query_rope,
    new_latent,
    new_rope,
    cache_latent,
    cache_rope,
    lengths,
    absorb_key,
    value_up,
    out_proj,
    gain_mix,
    gain_ffn_in,
    router,
    routes,
    expert_gate,
    expert_up,
    expert_down,
    shared_gate,
    shared_up,
    shared_down,
    gain_ffn_out,
):
    seq_count, width = hidden_in.shape
    heads, latent = query_nope.shape[1], cache_latent.shape[2]
    ep_count = lax.axis_size("ep")
    device_count = 2 * ep_count
    bits = (ep_count - 1).bit_length()
    grid_p = 2 ** ((bits + 1) // 2)
    grid_q = ep_count // grid_p
    positions = lengths.astype(jnp.float32)
    query_latent = jnp.einsum(
        "shn,chn->shc", query_nope, absorb_key, preferred_element_type=jnp.float32
    ).astype(jnp.bfloat16)
    query_pe = rotate(query_rope.astype(jnp.float32), positions[:, None, None]).astype(jnp.bfloat16)
    latent_new = normalize(new_latent.astype(jnp.float32)).astype(jnp.bfloat16)
    key_new = rotate(new_rope.astype(jnp.float32), positions[:, None]).astype(jnp.bfloat16)
    own_start = lax.axis_index("tp") * seq_count
    own_routes = lax.dynamic_slice_in_dim(routes, own_start, seq_count, 0)
    hot = jnp.any(
        own_routes[:, :, None] == lax.iota(jnp.int32, 128)[None, None, :], axis=1
    ).astype(jnp.bfloat16)
    own = jnp.concatenate([hidden_in, hot], axis=1)
    gains = jnp.stack([gain_mix, gain_ffn_in, gain_ffn_out])
    value_flat = value_up.reshape(value_up.shape[0], -1)
    bf = jnp.bfloat16
    score_scale = (query_nope.shape[-1] + query_rope.shape[-1]) ** (-0.5)
    sends = (grid_p - 1) + grid_p * (grid_q - 1) + ep_count
    big = pl.BlockSpec(memory_space=pl.ANY)
    near = pl.BlockSpec(memory_space=pltpu.VMEM)
    dma = pltpu.SemaphoreType.DMA
    total_rows = device_count * seq_count
    weights = (
        value_flat,
        out_proj,
        router,
        expert_gate[0],
        expert_up[0],
        expert_down[0],
        shared_gate,
        shared_up,
        shared_down,
    )
    operands = (
        query_latent,
        query_pe,
        latent_new,
        key_new,
        lengths,
        own,
        cache_latent,
        cache_rope,
        value_flat,
        out_proj,
        gains,
        router,
    ) + weights[3:]
    specs = (
        [near] * 4
        + [pl.BlockSpec(memory_space=pltpu.SMEM), near]
        + [big] * 4
        + [near]
        + [big] * 7
    )
    flops = 2 * total_rows * width * out_proj.shape[1]
    return pl.pallas_call(
        functools.partial(fused_kernel, grid_p, grid_q, score_scale),
        out_shape=jax.ShapeDtypeStruct((seq_count, width), bf),
        in_specs=specs,
        out_specs=near,
        scratch_shapes=[
            pltpu.VMEM(cache_latent.shape, bf),
            pltpu.VMEM(cache_rope.shape, bf),
        ]
        + [pltpu.VMEM(w.shape, bf) for w in weights]
        + [
            pltpu.VMEM((device_count,) + own.shape, bf),
            pltpu.VMEM((device_count, seq_count, out_proj.shape[0]), bf),
            pltpu.VMEM((device_count, total_rows, out_proj.shape[1]), bf),
            pltpu.VMEM((seq_count * heads, latent), bf),
            pltpu.VMEM((device_count, seq_count, width), bf),
            pltpu.VMEM((device_count, seq_count, width), bf),
            pltpu.VMEM((device_count, seq_count, width), bf),
            pltpu.VMEM((ep_count, seq_count, width), bf),
            pltpu.VMEM((ep_count, seq_count, width), bf),
            pltpu.VMEM((ep_count, seq_count, width), bf),
            dma((seq_count,)),
            dma((seq_count,)),
            dma((len(weights),)),
            dma((3, sends)),
            dma((3, device_count)),
            dma((ep_count,)),
            dma((ep_count,)),
            dma((ep_count,)),
            dma((ep_count,)),
        ],
        compiler_params=pltpu.CompilerParams(
            collective_id=0, has_side_effects=True, vmem_limit_bytes=56 * 2**20
        ),
        cost_estimate=pl.CostEstimate(flops=flops, bytes_accessed=2**24, transcendentals=0),
        name="layer_step",
    )(*operands)


def local(*args):
    hidden_in, out_proj, router = args[0], args[10], args[13]
    device_count = lax.axis_size("ep") * lax.axis_size("tp")
    fits = (
        lax.axis_size("tp") == 2
        and hidden_in.shape[0] == 8
        and device_count * hidden_in.shape[0] <= 256
        and out_proj.shape[1] % 128 == 0
        and router.shape[1] == device_count
    )
    return local_fused(*args) if fits else local_wide(*args)


def solution(mesh):
    placed = (
        P(("grp", "ep", "tp"), None),
        P(("grp", "ep", "tp"), None, None),
        P(("grp", "ep", "tp"), None, None),
        P(("grp", "ep", "tp"), None),
        P(("grp", "ep", "tp"), None),
        P(("grp", "ep", "tp"), None, None),
        P(("grp", "ep", "tp"), None, None),
        P(("grp", "ep", "tp")),
        P(),
        P(),
        P(None, ("ep", "tp")),
        P(),
        P(),
        P(),
        P(("grp", "ep"), None),
        P(("ep", "tp"), None, None),
        P(("ep", "tp"), None, None),
        P(("ep", "tp"), None, None),
        P(),
        P(),
        P(),
        P(),
    )
    return jax.shard_map(
        local, mesh=mesh, in_specs=placed, out_specs=P(("grp", "ep", "tp"), None), check_vma=False
    )
```

```python
import functools

import jax
import jax.numpy as jnp
from jax import lax
from jax.experimental import pallas as pl
from jax.experimental.pallas import tpu as pltpu
from jax.sharding import PartitionSpec as P

ABLK = 512


rope_theta = 10000.0
norm_eps = 1e-06
routed_scale = 2.5
masked_score = -1e30


def normalize(values):
    return values * lax.rsqrt(jnp.mean(values * values, axis=-1, keepdims=True) + norm_eps)


def rotate(values, positions):
    half_dim = values.shape[-1] // 2
    inverse = rope_theta ** (-jnp.arange(half_dim, dtype=jnp.float32) * 2.0 / values.shape[-1])
    angles = positions * inverse
    cosine = jnp.cos(angles)
    sine_table = jnp.sin(angles)
    first_half = values[..., :half_dim]
    second_half = values[..., half_dim:]
    return jnp.concatenate(
        [
            first_half * cosine - second_half * sine_table,
            first_half * sine_table + second_half * cosine,
        ],
        axis=-1,
    )


def swiglu(flat_rows, gate_w, up_w, down_w):
    gate_part = jnp.dot(flat_rows, gate_w, preferred_element_type=jnp.float32)
    up_part = jnp.dot(flat_rows, up_w, preferred_element_type=jnp.float32)
    inner_rows = (jax.nn.silu(gate_part) * up_part).astype(jnp.bfloat16)
    return jnp.dot(inner_rows, down_w, preferred_element_type=jnp.float32).astype(jnp.bfloat16)


def local_wide(
    hidden_in,
    query_nope,
    query_rope,
    new_latent,
    new_rope,
    cache_latent,
    cache_rope,
    lengths,
    absorb_key,
    value_up,
    out_proj,
    gain_mix,
    gain_ffn_in,
    router,
    routes,
    expert_gate,
    expert_up,
    expert_down,
    shared_gate,
    shared_up,
    shared_down,
    gain_ffn_out,
):
    seq_count = hidden_in.shape[0]
    positions = lengths.astype(jnp.float32)
    query_latent = jnp.einsum(
        "shn,chn->shc", query_nope, absorb_key, preferred_element_type=jnp.float32
    ).astype(jnp.bfloat16)
    query_pe = rotate(query_rope.astype(jnp.float32), positions[:, None, None]).astype(jnp.bfloat16)
    latent_new = normalize(new_latent.astype(jnp.float32)).astype(jnp.bfloat16)
    key_new = rotate(new_rope.astype(jnp.float32), positions[:, None]).astype(jnp.bfloat16)
    score_scale = (query_nope.shape[-1] + query_rope.shape[-1]) ** (-0.5)
    new_score = (
        jnp.einsum("shc,sc->sh", query_latent, latent_new, preferred_element_type=jnp.float32)
        + jnp.einsum("shr,sr->sh", query_pe, key_new, preferred_element_type=jnp.float32)
    ) * score_scale

    def attend_block(block_index, loop_state):
        running_max, weight_total, weighted_sum = loop_state
        block_start = block_index * ABLK
        block_latent = lax.dynamic_slice_in_dim(cache_latent, block_start, ABLK, 1)
        block_rope = lax.dynamic_slice_in_dim(cache_rope, block_start, ABLK, 1)
        scores = (
            jnp.einsum(
                "shc,skc->shk", query_latent, block_latent, preferred_element_type=jnp.float32
            )
            + jnp.einsum("shr,skr->shk", query_pe, block_rope, preferred_element_type=jnp.float32)
        ) * score_scale
        key_index = block_start + lax.iota(jnp.int32, ABLK)
        in_range = key_index[None, None, :] < lengths[:, None, None]
        scores = jnp.where(in_range, scores, masked_score)
        new_max = jnp.maximum(running_max, jnp.max(scores, axis=-1))
        rescale = jnp.exp(running_max - new_max)
        weights = jnp.exp(scores - new_max[..., None])
        weight_total = weight_total * rescale + jnp.sum(weights, axis=-1)
        weighted_sum = weighted_sum * rescale[..., None] + jnp.einsum(
            "shk,skc->shc",
            weights.astype(jnp.bfloat16),
            block_latent,
            preferred_element_type=jnp.float32,
        )
        return (new_max, weight_total, weighted_sum)

    longest = jnp.max(lengths)
    block_count = (longest + ABLK - 1) // ABLK
    ones_start = jnp.ones_like(new_score)
    sum_start = ones_start[..., None] * latent_new.astype(jnp.float32)[:, None, :]
    final_max, weight_total, weighted_sum = lax.fori_loop(
        0, block_count, attend_block, (new_score, ones_start, sum_start)
    )
    latent_out = (weighted_sum / weight_total[..., None]).astype(jnp.bfloat16)
    heads_out = (
        jnp.einsum("shc,chv->shv", latent_out, value_up, preferred_element_type=jnp.float32)
        .astype(jnp.bfloat16)
        .reshape(seq_count, -1)
    )
    column_rows = jnp.dot(
        lax.all_gather(heads_out, ("ep", "tp"), axis=0, tiled=True),
        out_proj,
        preferred_element_type=jnp.float32,
    ).astype(jnp.bfloat16)
    mixed_rows = lax.all_to_all(column_rows, ("ep", "tp"), split_axis=0, concat_axis=1, tiled=True)
    after_mix = (
        hidden_in.astype(jnp.float32)
        + gain_mix.astype(jnp.float32) * normalize(mixed_rows.astype(jnp.float32))
    ).astype(jnp.bfloat16)
    ffn_in = (normalize(after_mix.astype(jnp.float32)) * gain_ffn_in.astype(jnp.float32)).astype(
        jnp.bfloat16
    )
    affinity = jax.nn.sigmoid(jnp.dot(ffn_in, router, preferred_element_type=jnp.float32))
    experts_total = router.shape[1]
    own_start = lax.axis_index("tp") * seq_count
    own_routes = lax.dynamic_slice_in_dim(routes, own_start, seq_count, 0)
    choose = own_routes[..., None] == lax.iota(jnp.int32, experts_total)[None, None, :]
    chosen = jnp.sum(jnp.where(choose, affinity[:, None, :], 0.0), axis=-1)
    route_weights = chosen / jnp.sum(chosen, axis=-1, keepdims=True) * routed_scale
    group_rows, top_count = routes.shape
    capacity = 2 * ((group_rows * top_count + experts_total - 1) // experts_total)
    flat_routes = routes.reshape(-1)
    order_index = lax.iota(jnp.int32, group_rows * top_count)
    same_expert = flat_routes[:, None] == flat_routes[None, :]
    earlier = order_index[None, :] < order_index[:, None]
    slot_number = jnp.sum(jnp.logical_and(same_expert, earlier), axis=1)
    slot_number = slot_number.reshape(group_rows, top_count)
    own_slots = lax.dynamic_slice_in_dim(slot_number, own_start, seq_count, 0)
    slot_index = own_routes * capacity + own_slots
    slots_total = experts_total * capacity
    slot_table = jnp.any(
        slot_index[None, :, :] == lax.iota(jnp.int32, slots_total)[:, None, None], axis=-1
    ).astype(jnp.bfloat16)
    outgoing_terms = jnp.dot(slot_table, ffn_in, preferred_element_type=jnp.float32)
    outgoing = outgoing_terms.astype(jnp.bfloat16).reshape(experts_total, capacity, -1)
    received = lax.all_to_all(outgoing, ("ep", "tp"), split_axis=0, concat_axis=0, tiled=True)
    ep_count = lax.axis_size("ep")
    tp_count = lax.axis_size("tp")
    item_count = received.shape[1]
    width = received.shape[2]
    merged = jnp.sum(received.reshape(ep_count, tp_count, item_count, width), axis=1)
    outputs = swiglu(
        merged.reshape(ep_count * item_count, width), expert_gate[0], expert_up[0], expert_down[0]
    )
    copies = jnp.broadcast_to(
        outputs.reshape(ep_count, 1, item_count, width), (ep_count, tp_count, item_count, width)
    )
    copies = copies.reshape(ep_count * tp_count, item_count, width)
    returned = lax.all_to_all(copies, ("ep", "tp"), split_axis=0, concat_axis=0, tiled=True)
    picked = returned.reshape(slots_total, -1)[slot_index]
    routed = jnp.sum(picked.astype(jnp.float32) * route_weights[..., None], axis=1)
    shared = swiglu(ffn_in, shared_gate, shared_up, shared_down)
    combined = routed + shared.astype(jnp.float32)
    return (
        after_mix.astype(jnp.float32) + gain_ffn_out.astype(jnp.float32) * normalize(combined)
    ).astype(jnp.bfloat16)


def fused_kernel(
    grid_p,
    grid_q,
    score_scale,
    hidden_ref,
    qn_ref,
    qr_ref,
    nl_ref,
    nr_ref,
    len_ref,
    routes_ref,
    gm_ref,
    gf_ref,
    go_ref,
    ab_hbm,
    cl_hbm,
    cr_hbm,
    vup_hbm,
    wo_hbm,
    router_hbm,
    eg_hbm,
    eu_hbm,
    ed_hbm,
    sg_hbm,
    su_hbm,
    sd_hbm,
    out_ref,
    cl,
    cr,
    vup,
    wide_up,
    ql_ref,
    qp_ref,
    ab,
    vraw,
    wo,
    router,
    eg,
    eu,
    ed,
    sg,
    su,
    sd,
    xbuf,
    hbuf,
    cbuf,
    lat,
    norm_rows,
    mix_rows,
    terms,
    sib,
    part,
    back,
    cache_sem,
    rope_sem,
    weight_sem,
    ag_send,
    ag_recv,
    sib_send,
    sib_recv,
    back_send,
    back_recv,
):
    seq_count, heads, nope = qn_ref.shape
    rope = qr_ref.shape[2]
    width = out_ref.shape[1]
    ep_count = grid_p * grid_q
    device_count = 2 * ep_count
    total_rows = device_count * seq_count
    me_e = lax.axis_index("ep")
    me_t = lax.axis_index("tp")
    other_t = 1 - me_t
    p = me_e // grid_q
    q = me_e % grid_q
    me = me_e * 2 + me_t

    def device(e, t):
        return {"ep": e, "tp": t}

    sibling = device(me_e, other_t)
    barrier = pltpu.get_barrier_semaphore()
    for step in range(1, ep_count):
        pl.semaphore_signal(
            barrier,
            inc=1,
            device_id=device((me_e + step) % ep_count, me_t),
            device_id_type=pl.DeviceIdType.MESH,
        )
    pl.semaphore_signal(
        barrier, inc=1, device_id=sibling, device_id_type=pl.DeviceIdType.MESH
    )

    early_copies = []
    for index, (source, target) in enumerate(((ab_hbm, ab), (vup_hbm, vraw))):
        copy = pltpu.make_async_copy(source, target, weight_sem.at[index])
        copy.start()
        early_copies.append(copy)
    cache_copies = []
    for s in range(seq_count):
        pair = (
            pltpu.make_async_copy(cl_hbm.at[s], cl.at[s], cache_sem.at[s]),
            pltpu.make_async_copy(cr_hbm.at[s], cr.at[s], rope_sem.at[s]),
        )
        pair[0].start()
        pair[1].start()
        cache_copies.append(pair)
    weight_copies = []
    moves = (
        (wo_hbm, wo),
        (router_hbm, router),
        (eg_hbm, eg),
        (eu_hbm, eu),
        (ed_hbm, ed),
        (sg_hbm, sg),
        (su_hbm, su),
        (sd_hbm, sd),
    )
    for index, (source, target) in enumerate(moves):
        copy = pltpu.make_async_copy(source, target, weight_sem.at[index + 2])
        copy.start()
        weight_copies.append(copy)

    xbuf[me, :, 0:width] = hidden_ref[...]
    mark_shape = (seq_count, xbuf.shape[2] - width)
    mark_row = lax.broadcasted_iota(jnp.int32, mark_shape, 0)
    mark_lane = lax.broadcasted_iota(jnp.int32, mark_shape, 1)
    marks = jnp.zeros(mark_shape, jnp.float32)
    for s in range(seq_count):
        for j in range(routes_ref.shape[0]):
            expert = routes_ref[j, me_t * seq_count + s]
            marks = jnp.where((mark_row == s) & (mark_lane == expert), 1.0, marks)
    xbuf[me, :, width:] = marks.astype(jnp.bfloat16)

    half = rope // 2
    turn_row = lax.broadcasted_iota(jnp.int32, (seq_count, rope), 0)
    turn_lane = lax.broadcasted_iota(jnp.int32, (seq_count, rope), 1)
    position = jnp.zeros((seq_count, rope), jnp.float32)
    for s in range(seq_count):
        position = jnp.where(turn_row == s, len_ref[s].astype(jnp.float32), position)
    inverse = jnp.zeros((seq_count, rope), jnp.float32)
    for i in range(half):
        inverse = jnp.where(turn_lane % half == i, rope_theta ** (-2.0 * i / rope), inverse)
    angles = position * inverse
    cosine = jnp.cos(angles)
    sine = jnp.sin(angles) * jnp.where(turn_lane < half, -1.0, 1.0)

    def turned(values, cos_rows, sin_rows):
        swapped = jnp.concatenate([values[:, half:], values[:, :half]], axis=1)
        return values * cos_rows + swapped * sin_rows

    def per_head(table):
        return jnp.broadcast_to(table[:, None, :], (seq_count, heads, rope)).reshape(
            seq_count * heads, rope
        )

    query_rows = qr_ref[...].astype(jnp.float32).reshape(seq_count * heads, rope)
    qp_ref[...] = turned(query_rows, per_head(cosine), per_head(sine)).astype(jnp.bfloat16)
    key_rows = turned(nr_ref[...].astype(jnp.float32), cosine, sine).astype(jnp.bfloat16)
    key_rows = key_rows.astype(jnp.float32)
    new_rows = normalize(nl_ref[...].astype(jnp.float32)).astype(jnp.bfloat16).astype(jnp.float32)

    nope_rows = qn_ref[...].astype(jnp.float32).reshape(seq_count * heads, nope)
    row_head = lax.broadcasted_iota(jnp.int32, (seq_count * heads, 2 * nope), 0) % heads
    pair_lane = lax.broadcasted_iota(jnp.int32, (seq_count * heads, 2 * nope), 1) // nope
    doubled = jnp.concatenate([nope_rows, nope_rows], axis=1)
    spread_query = jnp.concatenate(
        [
            jnp.where(row_head == pair_lane + 2 * j, doubled, 0.0).astype(jnp.bfloat16)
            for j in range(heads // 2)
        ],
        axis=1,
    )
    early_copies[0].wait()
    ql_ref[...] = jnp.dot(spread_query, ab[...], preferred_element_type=jnp.float32).astype(
        jnp.bfloat16
    )

    line_steps = list(range(1, grid_p))
    pending = []

    class Gather:
        def __init__(self, buf, which):
            self.buf, self.which, self.count = buf, which, 0

        def send(self, slot, target):
            copy = pltpu.make_async_remote_copy(
                src_ref=self.buf.at[slot],
                dst_ref=self.buf.at[slot],
                send_sem=ag_send.at[self.which, self.count],
                recv_sem=ag_recv.at[self.which, slot],
                device_id=target,
                device_id_type=pl.DeviceIdType.MESH,
            )
            copy.start()
            pending.append(copy)
            self.count += 1

        def arrive(self, slot):
            pltpu.make_async_remote_copy(
                src_ref=self.buf.at[slot],
                dst_ref=self.buf.at[slot],
                send_sem=ag_send.at[self.which, 0],
                recv_sem=ag_recv.at[self.which, slot],
                device_id=sibling,
                device_id_type=pl.DeviceIdType.MESH,
            ).wait_recv()

        def line(self, step):
            return (p + step) % grid_p

        def first(self):
            for step in sorted(line_steps, key=lambda v: -min(v, grid_p - v)):
                self.send(me, device(self.line(step) * grid_q + q, me_t))
            for turn in range(1, grid_q):
                self.send(me, device(p * grid_q + (q + turn) % grid_q, me_t))
            self.send(me, sibling)

        def second(self):
            for step in sorted(line_steps, key=lambda v: min(v, grid_p - v)):
                slot = (self.line(step) * grid_q + q) * 2 + me_t
                self.arrive(slot)
                for turn in range(1, grid_q):
                    self.send(slot, device(p * grid_q + (q + turn) % grid_q, me_t))
                self.send(slot, sibling)

        def third(self):
            for step in sorted([0] + line_steps, key=lambda v: min(v, grid_p - v)):
                for turn in range(1, grid_q):
                    slot = (self.line(step) * grid_q + (q + turn) % grid_q) * 2 + me_t
                    self.arrive(slot)
                    self.send(slot, sibling)

        def last(self):
            for e in range(ep_count):
                self.arrive(e * 2 + other_t)

    context = cl.shape[1]
    key_index = lax.broadcasted_iota(jnp.int32, (heads, context), 1)

    def attend(s):
        cache_copies[s][0].wait()
        cache_copies[s][1].wait()
        q_lat = ql_ref[s * heads : (s + 1) * heads, :]
        q_pe = qp_ref[s * heads : (s + 1) * heads, :]
        keys = cl[s]
        dims = (((1,), (1,)), ((), ()))
        scores = (
            lax.dot_general(q_lat, keys, dims, preferred_element_type=jnp.float32)
            + jnp.dot(q_pe, cr[s], preferred_element_type=jnp.float32)
        ) * score_scale
        new_row = new_rows[s : s + 1, :]
        key_row = key_rows[s : s + 1, :]
        new_score = (
            jnp.sum(q_lat.astype(jnp.float32) * new_row, axis=-1, keepdims=True)
            + jnp.sum(q_pe.astype(jnp.float32) * key_row, axis=-1, keepdims=True)
        ) * score_scale
        scores = jnp.where(key_index < len_ref[s], scores, masked_score)
        row_max = jnp.maximum(jnp.max(scores, axis=-1, keepdims=True), new_score)
        weights = jnp.exp(scores - row_max)
        new_weight = jnp.exp(new_score - row_max)
        weight_total = jnp.sum(weights, axis=-1, keepdims=True) + new_weight
        weighted = jnp.dot(weights.astype(jnp.bfloat16), keys, preferred_element_type=jnp.float32)
        weighted = weighted + new_weight.astype(jnp.bfloat16).astype(jnp.float32) * new_row
        lat[s * heads : (s + 1) * heads, :] = (weighted / weight_total).astype(jnp.bfloat16)

    rows_gather = Gather(xbuf, 0)
    cut_a, cut_b = seq_count // 2, seq_count - seq_count // 4
    for s in range(cut_a):
        attend(s)
    early_copies[1].wait()
    value_dim = vraw.shape[2]
    wide_up[...] = vraw[...].astype(jnp.float32)
    for h in range(heads):
        vup[:, h * value_dim : (h + 1) * value_dim] = wide_up[:, h, :].astype(jnp.bfloat16)
    pl.semaphore_wait(barrier, ep_count)
    rows_gather.first()
    for s in range(cut_a, cut_b):
        attend(s)
    rows_gather.second()
    for s in range(cut_b, seq_count):
        attend(s)

    spread = jnp.dot(lat[...], vup[...], preferred_element_type=jnp.float32)
    own_heads = []
    head_row = lax.broadcasted_iota(jnp.int32, (seq_count, heads, value_dim), 1)
    for h in range(heads):
        block = spread[:, h * value_dim : (h + 1) * value_dim].reshape(seq_count, heads, value_dim)
        own_heads.append(jnp.sum(jnp.where(head_row == h, block, 0.0), axis=1))
    hbuf[me] = jnp.concatenate(own_heads, axis=1).astype(jnp.bfloat16)
    heads_gather = Gather(hbuf, 1)
    heads_gather.first()
    rows_gather.third()
    heads_gather.second()
    heads_gather.third()
    rows_gather.last()
    weight_copies[0].wait()
    heads_gather.last()

    flat_heads = hbuf[...].reshape(total_rows, hbuf.shape[2])
    cbuf[me] = jnp.dot(flat_heads, wo[...], preferred_element_type=jnp.float32).astype(jnp.bfloat16)
    columns_gather = Gather(cbuf, 2)
    columns_gather.first()
    columns_gather.second()
    columns_gather.third()
    columns_gather.last()

    gains = [
        ref[...].astype(jnp.float32).reshape(1, width) for ref in (gm_ref, gf_ref, go_ref)
    ]
    mixed = jnp.concatenate([cbuf[o] for o in range(device_count)], axis=1).astype(jnp.float32)
    stage = xbuf[...].reshape(total_rows, xbuf.shape[2])
    after_mix = (stage[:, :width].astype(jnp.float32) + gains[0] * normalize(mixed)).astype(
        jnp.bfloat16
    )
    mix_rows[...] = after_mix.reshape(mix_rows.shape)
    ffn_in = (normalize(after_mix.astype(jnp.float32)) * gains[1]).astype(jnp.bfloat16)
    norm_rows[...] = ffn_in.reshape(norm_rows.shape)
    weight_copies[1].wait()
    affinity = jax.nn.sigmoid(
        lax.dot_general(
            ffn_in, router[...], (((1,), (1,)), ((), ())), preferred_element_type=jnp.float32
        )
    )
    hot = stage[:, width : width + affinity.shape[1]].astype(jnp.float32)
    chosen = affinity * hot
    lane = lax.broadcasted_iota(jnp.int32, chosen.shape, 1)
    mine = jnp.sum(jnp.where(lane == me, chosen, 0.0), axis=1, keepdims=True)
    mine = mine / jnp.sum(chosen, axis=1, keepdims=True) * routed_scale
    for copy in weight_copies[2:5]:
        copy.wait()
    expert_out = swiglu(ffn_in, eg[...], eu[...], ed[...])
    scaled = (expert_out.astype(jnp.float32) * mine).astype(jnp.bfloat16)
    terms[...] = scaled.reshape(terms.shape)

    def to_sibling(step):
        e = (me_e + step) % ep_count
        return pltpu.make_async_remote_copy(
            src_ref=terms.at[e * 2 + other_t],
            dst_ref=sib.at[e],
            send_sem=sib_send.at[step],
            recv_sem=sib_recv.at[e],
            device_id=sibling,
            device_id_type=pl.DeviceIdType.MESH,
        )

    order = sorted(range(1, ep_count), key=lambda v: -min(v, ep_count - v)) + [0]
    sib_copies = [to_sibling(step) for step in order]
    for copy in sib_copies:
        copy.start()
    sends = []
    for step in order:
        e = (me_e + step) % ep_count
        to_sibling(step).wait_recv()
        paired = terms[e * 2 + me_t].astype(jnp.float32) + sib[e].astype(jnp.float32)
        if step == 0:
            routed = paired
        else:
            part[e] = paired.astype(jnp.bfloat16)
            copy = pltpu.make_async_remote_copy(
                src_ref=part.at[e],
                dst_ref=back.at[me_e],
                send_sem=back_send.at[step],
                recv_sem=back_recv.at[me_e],
                device_id=device(e, me_t),
                device_id_type=pl.DeviceIdType.MESH,
            )
            copy.start()
            sends.append(copy)
    for copy in weight_copies[5:8]:
        copy.wait()
    combined = routed + swiglu(norm_rows[me], sg[...], su[...], sd[...]).astype(jnp.float32)
    for step in reversed(order[:-1]):
        e = (me_e + step) % ep_count
        pltpu.make_async_remote_copy(
            src_ref=part.at[e],
            dst_ref=back.at[e],
            send_sem=back_send.at[step],
            recv_sem=back_recv.at[e],
            device_id=device(e, me_t),
            device_id_type=pl.DeviceIdType.MESH,
        ).wait_recv()
        combined = combined + back[e].astype(jnp.float32)
    out_ref[...] = (
        mix_rows[me].astype(jnp.float32) + gains[2] * normalize(combined)
    ).astype(jnp.bfloat16)
    for copy in pending + sib_copies + sends:
        copy.wait_send()


def local_fused(
    hidden_in,
    query_nope,
    query_rope,
    new_latent,
    new_rope,
    cache_latent,
    cache_rope,
    lengths,
    absorb_key,
    value_up,
    out_proj,
    gain_mix,
    gain_ffn_in,
    router,
    routes,
    expert_gate,
    expert_up,
    expert_down,
    shared_gate,
    shared_up,
    shared_down,
    gain_ffn_out,
):
    seq_count, width = hidden_in.shape
    heads, latent = query_nope.shape[1], cache_latent.shape[2]
    ep_count = lax.axis_size("ep")
    device_count = 2 * ep_count
    bits = (ep_count - 1).bit_length()
    grid_p = 2 ** ((bits + 1) // 2)
    grid_q = ep_count // grid_p
    bf = jnp.bfloat16
    score_scale = (query_nope.shape[-1] + query_rope.shape[-1]) ** (-0.5)
    sends = (grid_p - 1) + grid_p * (grid_q - 1) + ep_count
    big = pl.BlockSpec(memory_space=pl.ANY)
    near = pl.BlockSpec(memory_space=pltpu.VMEM)
    dma = pltpu.SemaphoreType.DMA
    total_rows = device_count * seq_count
    rope_rows = jnp.swapaxes(cache_rope, 1, 2)
    router_rows = jnp.swapaxes(router, 0, 1)
    absorb_rows = jnp.transpose(absorb_key, (1, 2, 0)).reshape(-1, latent)
    own_shape = (seq_count, width + 128)
    weights = (
        out_proj,
        router_rows,
        expert_gate[0],
        expert_up[0],
        expert_down[0],
        shared_gate,
        shared_up,
        shared_down,
    )
    operands = (
        hidden_in,
        query_nope,
        query_rope,
        new_latent,
        new_rope,
        lengths,
        jnp.swapaxes(routes, 0, 1),
        gain_mix,
        gain_ffn_in,
        gain_ffn_out,
        absorb_rows,
        cache_latent,
        rope_rows,
        value_up,
    ) + weights
    scalar = pl.BlockSpec(memory_space=pltpu.SMEM)
    specs = [near] * 5 + [scalar] * 2 + [near] * 3 + [big] * 12
    flops = 2 * total_rows * width * out_proj.shape[1]
    return pl.pallas_call(
        functools.partial(fused_kernel, grid_p, grid_q, score_scale),
        out_shape=jax.ShapeDtypeStruct((seq_count, width), bf),
        in_specs=specs,
        out_specs=near,
        scratch_shapes=[
            pltpu.VMEM(cache_latent.shape, bf),
            pltpu.VMEM(rope_rows.shape, bf),
            pltpu.VMEM((latent, value_up.shape[1] * value_up.shape[2]), bf),
            pltpu.VMEM(value_up.shape, jnp.float32),
            pltpu.VMEM((seq_count * heads, latent), bf),
            pltpu.VMEM((seq_count * heads, query_rope.shape[2]), bf),
            pltpu.VMEM(absorb_rows.shape, bf),
            pltpu.VMEM(value_up.shape, bf),
        ]
        + [pltpu.VMEM(w.shape, bf) for w in weights]
        + [
            pltpu.VMEM((device_count,) + own_shape, bf),
            pltpu.VMEM((device_count, seq_count, out_proj.shape[0]), bf),
            pltpu.VMEM((device_count, total_rows, out_proj.shape[1]), bf),
            pltpu.VMEM((seq_count * heads, latent), bf),
            pltpu.VMEM((device_count, seq_count, width), bf),
            pltpu.VMEM((device_count, seq_count, width), bf),
            pltpu.VMEM((device_count, seq_count, width), bf),
            pltpu.VMEM((ep_count, seq_count, width), bf),
            pltpu.VMEM((ep_count, seq_count, width), bf),
            pltpu.VMEM((ep_count, seq_count, width), bf),
            dma((seq_count,)),
            dma((seq_count,)),
            dma((len(weights) + 2,)),
            dma((3, sends)),
            dma((3, device_count)),
            dma((ep_count,)),
            dma((ep_count,)),
            dma((ep_count,)),
            dma((ep_count,)),
        ],
        compiler_params=pltpu.CompilerParams(
            collective_id=0, has_side_effects=True, vmem_limit_bytes=56 * 2**20
        ),
        cost_estimate=pl.CostEstimate(flops=flops, bytes_accessed=2**24, transcendentals=0),
        name="layer_step",
    )(*operands)


def local(*args):
    hidden_in, out_proj, router = args[0], args[10], args[13]
    device_count = lax.axis_size("ep") * lax.axis_size("tp")
    fits = (
        lax.axis_size("tp") == 2
        and hidden_in.shape[0] == 8
        and device_count * hidden_in.shape[0] <= 256
        and out_proj.shape[1] % 128 == 0
        and router.shape[1] == device_count
    )
    return local_fused(*args) if fits else local_wide(*args)


def solution(mesh):
    placed = (
        P(("grp", "ep", "tp"), None),
        P(("grp", "ep", "tp"), None, None),
        P(("grp", "ep", "tp"), None, None),
        P(("grp", "ep", "tp"), None),
        P(("grp", "ep", "tp"), None),
        P(("grp", "ep", "tp"), None, None),
        P(("grp", "ep", "tp"), None, None),
        P(("grp", "ep", "tp")),
        P(),
        P(),
        P(None, ("ep", "tp")),
        P(),
        P(),
        P(),
        P(("grp", "ep"), None),
        P(("ep", "tp"), None, None),
        P(("ep", "tp"), None, None),
        P(("ep", "tp"), None, None),
        P(),
        P(),
        P(),
        P(),
    )
    return jax.shard_map(
        local, mesh=mesh, in_specs=placed, out_specs=P(("grp", "ep", "tp"), None), check_vma=False
    )
```

```python
import functools

import jax
import jax.numpy as jnp
from jax import lax
from jax.experimental import pallas as pl
from jax.experimental.pallas import tpu as pltpu
from jax.sharding import PartitionSpec as P

ABLK = 512


rope_theta = 10000.0
norm_eps = 1e-06
routed_scale = 2.5
masked_score = -1e30


def normalize(values):
    return values * lax.rsqrt(jnp.mean(values * values, axis=-1, keepdims=True) + norm_eps)


def rotate(values, positions):
    half_dim = values.shape[-1] // 2
    inverse = rope_theta ** (-jnp.arange(half_dim, dtype=jnp.float32) * 2.0 / values.shape[-1])
    angles = positions * inverse
    cosine = jnp.cos(angles)
    sine_table = jnp.sin(angles)
    first_half = values[..., :half_dim]
    second_half = values[..., half_dim:]
    return jnp.concatenate(
        [
            first_half * cosine - second_half * sine_table,
            first_half * sine_table + second_half * cosine,
        ],
        axis=-1,
    )


def swiglu(flat_rows, gate_w, up_w, down_w):
    gate_part = jnp.dot(flat_rows, gate_w, preferred_element_type=jnp.float32)
    up_part = jnp.dot(flat_rows, up_w, preferred_element_type=jnp.float32)
    inner_rows = (jax.nn.silu(gate_part) * up_part).astype(jnp.bfloat16)
    return jnp.dot(inner_rows, down_w, preferred_element_type=jnp.float32).astype(jnp.bfloat16)


def local_wide(
    hidden_in,
    query_nope,
    query_rope,
    new_latent,
    new_rope,
    cache_latent,
    cache_rope,
    lengths,
    absorb_key,
    value_up,
    out_proj,
    gain_mix,
    gain_ffn_in,
    router,
    routes,
    expert_gate,
    expert_up,
    expert_down,
    shared_gate,
    shared_up,
    shared_down,
    gain_ffn_out,
):
    seq_count = hidden_in.shape[0]
    positions = lengths.astype(jnp.float32)
    query_latent = jnp.einsum(
        "shn,chn->shc", query_nope, absorb_key, preferred_element_type=jnp.float32
    ).astype(jnp.bfloat16)
    query_pe = rotate(query_rope.astype(jnp.float32), positions[:, None, None]).astype(jnp.bfloat16)
    latent_new = normalize(new_latent.astype(jnp.float32)).astype(jnp.bfloat16)
    key_new = rotate(new_rope.astype(jnp.float32), positions[:, None]).astype(jnp.bfloat16)
    score_scale = (query_nope.shape[-1] + query_rope.shape[-1]) ** (-0.5)
    new_score = (
        jnp.einsum("shc,sc->sh", query_latent, latent_new, preferred_element_type=jnp.float32)
        + jnp.einsum("shr,sr->sh", query_pe, key_new, preferred_element_type=jnp.float32)
    ) * score_scale

    def attend_block(block_index, loop_state):
        running_max, weight_total, weighted_sum = loop_state
        block_start = block_index * ABLK
        block_latent = lax.dynamic_slice_in_dim(cache_latent, block_start, ABLK, 1)
        block_rope = lax.dynamic_slice_in_dim(cache_rope, block_start, ABLK, 1)
        scores = (
            jnp.einsum(
                "shc,skc->shk", query_latent, block_latent, preferred_element_type=jnp.float32
            )
            + jnp.einsum("shr,skr->shk", query_pe, block_rope, preferred_element_type=jnp.float32)
        ) * score_scale
        key_index = block_start + lax.iota(jnp.int32, ABLK)
        in_range = key_index[None, None, :] < lengths[:, None, None]
        scores = jnp.where(in_range, scores, masked_score)
        new_max = jnp.maximum(running_max, jnp.max(scores, axis=-1))
        rescale = jnp.exp(running_max - new_max)
        weights = jnp.exp(scores - new_max[..., None])
        weight_total = weight_total * rescale + jnp.sum(weights, axis=-1)
        weighted_sum = weighted_sum * rescale[..., None] + jnp.einsum(
            "shk,skc->shc",
            weights.astype(jnp.bfloat16),
            block_latent,
            preferred_element_type=jnp.float32,
        )
        return (new_max, weight_total, weighted_sum)

    longest = jnp.max(lengths)
    block_count = (longest + ABLK - 1) // ABLK
    ones_start = jnp.ones_like(new_score)
    sum_start = ones_start[..., None] * latent_new.astype(jnp.float32)[:, None, :]
    final_max, weight_total, weighted_sum = lax.fori_loop(
        0, block_count, attend_block, (new_score, ones_start, sum_start)
    )
    latent_out = (weighted_sum / weight_total[..., None]).astype(jnp.bfloat16)
    heads_out = (
        jnp.einsum("shc,chv->shv", latent_out, value_up, preferred_element_type=jnp.float32)
        .astype(jnp.bfloat16)
        .reshape(seq_count, -1)
    )
    column_rows = jnp.dot(
        lax.all_gather(heads_out, ("ep", "tp"), axis=0, tiled=True),
        out_proj,
        preferred_element_type=jnp.float32,
    ).astype(jnp.bfloat16)
    mixed_rows = lax.all_to_all(column_rows, ("ep", "tp"), split_axis=0, concat_axis=1, tiled=True)
    after_mix = (
        hidden_in.astype(jnp.float32)
        + gain_mix.astype(jnp.float32) * normalize(mixed_rows.astype(jnp.float32))
    ).astype(jnp.bfloat16)
    ffn_in = (normalize(after_mix.astype(jnp.float32)) * gain_ffn_in.astype(jnp.float32)).astype(
        jnp.bfloat16
    )
    affinity = jax.nn.sigmoid(jnp.dot(ffn_in, router, preferred_element_type=jnp.float32))
    experts_total = router.shape[1]
    own_start = lax.axis_index("tp") * seq_count
    own_routes = lax.dynamic_slice_in_dim(routes, own_start, seq_count, 0)
    choose = own_routes[..., None] == lax.iota(jnp.int32, experts_total)[None, None, :]
    chosen = jnp.sum(jnp.where(choose, affinity[:, None, :], 0.0), axis=-1)
    route_weights = chosen / jnp.sum(chosen, axis=-1, keepdims=True) * routed_scale
    group_rows, top_count = routes.shape
    capacity = 2 * ((group_rows * top_count + experts_total - 1) // experts_total)
    flat_routes = routes.reshape(-1)
    order_index = lax.iota(jnp.int32, group_rows * top_count)
    same_expert = flat_routes[:, None] == flat_routes[None, :]
    earlier = order_index[None, :] < order_index[:, None]
    slot_number = jnp.sum(jnp.logical_and(same_expert, earlier), axis=1)
    slot_number = slot_number.reshape(group_rows, top_count)
    own_slots = lax.dynamic_slice_in_dim(slot_number, own_start, seq_count, 0)
    slot_index = own_routes * capacity + own_slots
    slots_total = experts_total * capacity
    slot_table = jnp.any(
        slot_index[None, :, :] == lax.iota(jnp.int32, slots_total)[:, None, None], axis=-1
    ).astype(jnp.bfloat16)
    outgoing_terms = jnp.dot(slot_table, ffn_in, preferred_element_type=jnp.float32)
    outgoing = outgoing_terms.astype(jnp.bfloat16).reshape(experts_total, capacity, -1)
    received = lax.all_to_all(outgoing, ("ep", "tp"), split_axis=0, concat_axis=0, tiled=True)
    ep_count = lax.axis_size("ep")
    tp_count = lax.axis_size("tp")
    item_count = received.shape[1]
    width = received.shape[2]
    merged = jnp.sum(received.reshape(ep_count, tp_count, item_count, width), axis=1)
    outputs = swiglu(
        merged.reshape(ep_count * item_count, width), expert_gate[0], expert_up[0], expert_down[0]
    )
    copies = jnp.broadcast_to(
        outputs.reshape(ep_count, 1, item_count, width), (ep_count, tp_count, item_count, width)
    )
    copies = copies.reshape(ep_count * tp_count, item_count, width)
    returned = lax.all_to_all(copies, ("ep", "tp"), split_axis=0, concat_axis=0, tiled=True)
    picked = returned.reshape(slots_total, -1)[slot_index]
    routed = jnp.sum(picked.astype(jnp.float32) * route_weights[..., None], axis=1)
    shared = swiglu(ffn_in, shared_gate, shared_up, shared_down)
    combined = routed + shared.astype(jnp.float32)
    return (
        after_mix.astype(jnp.float32) + gain_ffn_out.astype(jnp.float32) * normalize(combined)
    ).astype(jnp.bfloat16)


def fused_kernel(
    grid_p,
    grid_q,
    score_scale,
    hidden_ref,
    qn_ref,
    qr_ref,
    nl_ref,
    nr_ref,
    len_ref,
    routes_ref,
    gm_ref,
    gf_ref,
    go_ref,
    ab_hbm,
    cl_hbm,
    cr_hbm,
    vup_hbm,
    wo_hbm,
    router_hbm,
    eg_hbm,
    eu_hbm,
    ed_hbm,
    sg_hbm,
    su_hbm,
    sd_hbm,
    out_ref,
    cl,
    cr,
    vup,
    wide_up,
    ql_ref,
    qp_ref,
    ab,
    vraw,
    wo,
    router,
    eg,
    eu,
    ed,
    sg,
    su,
    sd,
    xbuf,
    hbuf,
    cbuf,
    lat,
    norm_rows,
    mix_rows,
    terms,
    sib,
    part,
    back,
    cache_sem,
    rope_sem,
    weight_sem,
    ag_send,
    ag_recv,
    sib_send,
    sib_recv,
    back_send,
    back_recv,
):
    seq_count, heads, nope = qn_ref.shape
    rope = qr_ref.shape[2]
    width = out_ref.shape[1]
    ep_count = grid_p * grid_q
    device_count = 2 * ep_count
    total_rows = device_count * seq_count
    me_e = lax.axis_index("ep")
    me_t = lax.axis_index("tp")
    other_t = 1 - me_t
    p = me_e // grid_q
    q = me_e % grid_q
    me = me_e * 2 + me_t

    def device(e, t):
        return {"ep": e, "tp": t}

    sibling = device(me_e, other_t)
    barrier = pltpu.get_barrier_semaphore()
    for step in range(1, ep_count):
        pl.semaphore_signal(
            barrier,
            inc=1,
            device_id=device((me_e + step) % ep_count, me_t),
            device_id_type=pl.DeviceIdType.MESH,
        )
    pl.semaphore_signal(
        barrier, inc=1, device_id=sibling, device_id_type=pl.DeviceIdType.MESH
    )

    early_copies = []
    for index, (source, target) in enumerate(((ab_hbm, ab), (vup_hbm, vraw))):
        copy = pltpu.make_async_copy(source, target, weight_sem.at[index])
        copy.start()
        early_copies.append(copy)
    cache_copies = []
    for s in range(seq_count):
        pair = (
            pltpu.make_async_copy(cl_hbm.at[s], cl.at[s], cache_sem.at[s]),
            pltpu.make_async_copy(cr_hbm.at[s], cr.at[s], rope_sem.at[s]),
        )
        pair[0].start()
        pair[1].start()
        cache_copies.append(pair)
    weight_copies = []
    moves = (
        (wo_hbm, wo),
        (router_hbm, router),
        (eg_hbm, eg),
        (eu_hbm, eu),
        (ed_hbm, ed),
        (sg_hbm, sg),
        (su_hbm, su),
        (sd_hbm, sd),
    )
    for index, (source, target) in enumerate(moves):
        copy = pltpu.make_async_copy(source, target, weight_sem.at[index + 2])
        copy.start()
        weight_copies.append(copy)

    xbuf[me, :, 0:width] = hidden_ref[...]
    mark_shape = (seq_count, xbuf.shape[2] - width)
    mark_row = lax.broadcasted_iota(jnp.int32, mark_shape, 0)
    mark_lane = lax.broadcasted_iota(jnp.int32, mark_shape, 1)
    marks = jnp.zeros(mark_shape, jnp.float32)
    for s in range(seq_count):
        for j in range(routes_ref.shape[0]):
            expert = routes_ref[j, me_t * seq_count + s]
            marks = jnp.where((mark_row == s) & (mark_lane == expert), 1.0, marks)
    xbuf[me, :, width:] = marks.astype(jnp.bfloat16)

    line_steps = list(range(1, grid_p))
    pending = []

    class Gather:
        def __init__(self, buf, which):
            self.buf, self.which, self.count = buf, which, 0

        def send(self, slot, target):
            copy = pltpu.make_async_remote_copy(
                src_ref=self.buf.at[slot],
                dst_ref=self.buf.at[slot],
                send_sem=ag_send.at[self.which, self.count],
                recv_sem=ag_recv.at[self.which, slot],
                device_id=target,
                device_id_type=pl.DeviceIdType.MESH,
            )
            copy.start()
            pending.append(copy)
            self.count += 1

        def arrive(self, slot):
            pltpu.make_async_remote_copy(
                src_ref=self.buf.at[slot],
                dst_ref=self.buf.at[slot],
                send_sem=ag_send.at[self.which, 0],
                recv_sem=ag_recv.at[self.which, slot],
                device_id=sibling,
                device_id_type=pl.DeviceIdType.MESH,
            ).wait_recv()

        def line(self, step):
            return (p + step) % grid_p

        def first(self):
            for step in sorted(line_steps, key=lambda v: -min(v, grid_p - v)):
                self.send(me, device(self.line(step) * grid_q + q, me_t))
            for turn in range(1, grid_q):
                self.send(me, device(p * grid_q + (q + turn) % grid_q, me_t))
            self.send(me, sibling)

        def second(self):
            for step in sorted(line_steps, key=lambda v: min(v, grid_p - v)):
                slot = (self.line(step) * grid_q + q) * 2 + me_t
                self.arrive(slot)
                for turn in range(1, grid_q):
                    self.send(slot, device(p * grid_q + (q + turn) % grid_q, me_t))
                self.send(slot, sibling)

        def third(self):
            for step in sorted([0] + line_steps, key=lambda v: min(v, grid_p - v)):
                for turn in range(1, grid_q):
                    slot = (self.line(step) * grid_q + (q + turn) % grid_q) * 2 + me_t
                    self.arrive(slot)
                    self.send(slot, sibling)

        def last(self):
            for e in range(ep_count):
                self.arrive(e * 2 + other_t)

    rows_gather = Gather(xbuf, 0)
    pl.semaphore_wait(barrier, ep_count)
    rows_gather.first()

    half = rope // 2
    turn_row = lax.broadcasted_iota(jnp.int32, (seq_count, rope), 0)
    turn_lane = lax.broadcasted_iota(jnp.int32, (seq_count, rope), 1)
    position = jnp.zeros((seq_count, rope), jnp.float32)
    for s in range(seq_count):
        position = jnp.where(turn_row == s, len_ref[s].astype(jnp.float32), position)
    inverse = jnp.zeros((seq_count, rope), jnp.float32)
    for i in range(half):
        inverse = jnp.where(turn_lane % half == i, rope_theta ** (-2.0 * i / rope), inverse)
    angles = position * inverse
    cosine = jnp.cos(angles)
    sine = jnp.sin(angles) * jnp.where(turn_lane < half, -1.0, 1.0)

    def turned(values, cos_rows, sin_rows):
        swapped = jnp.concatenate([values[:, half:], values[:, :half]], axis=1)
        return values * cos_rows + swapped * sin_rows

    def per_head(table):
        return jnp.broadcast_to(table[:, None, :], (seq_count, heads, rope)).reshape(
            seq_count * heads, rope
        )

    query_rows = qr_ref[...].astype(jnp.float32).reshape(seq_count * heads, rope)
    qp_ref[...] = turned(query_rows, per_head(cosine), per_head(sine)).astype(jnp.bfloat16)
    key_rows = turned(nr_ref[...].astype(jnp.float32), cosine, sine).astype(jnp.bfloat16)
    key_rows = key_rows.astype(jnp.float32)
    new_rows = normalize(nl_ref[...].astype(jnp.float32)).astype(jnp.bfloat16).astype(jnp.float32)

    nope_rows = qn_ref[...].astype(jnp.float32).reshape(seq_count * heads, nope)
    row_head = lax.broadcasted_iota(jnp.int32, (seq_count * heads, 2 * nope), 0) % heads
    pair_lane = lax.broadcasted_iota(jnp.int32, (seq_count * heads, 2 * nope), 1) // nope
    doubled = jnp.concatenate([nope_rows, nope_rows], axis=1)
    spread_query = jnp.concatenate(
        [
            jnp.where(row_head == pair_lane + 2 * j, doubled, 0.0).astype(jnp.bfloat16)
            for j in range(heads // 2)
        ],
        axis=1,
    )
    early_copies[0].wait()
    ql_ref[...] = jnp.dot(spread_query, ab[...], preferred_element_type=jnp.float32).astype(
        jnp.bfloat16
    )

    context = cl.shape[1]
    key_index = lax.broadcasted_iota(jnp.int32, (heads, context), 1)

    def attend(s):
        cache_copies[s][0].wait()
        cache_copies[s][1].wait()
        q_lat = ql_ref[s * heads : (s + 1) * heads, :]
        q_pe = qp_ref[s * heads : (s + 1) * heads, :]
        keys = cl[s]
        dims = (((1,), (1,)), ((), ()))
        scores = (
            lax.dot_general(q_lat, keys, dims, preferred_element_type=jnp.float32)
            + jnp.dot(q_pe, cr[s], preferred_element_type=jnp.float32)
        ) * score_scale
        new_row = new_rows[s : s + 1, :]
        key_row = key_rows[s : s + 1, :]
        new_score = (
            jnp.sum(q_lat.astype(jnp.float32) * new_row, axis=-1, keepdims=True)
            + jnp.sum(q_pe.astype(jnp.float32) * key_row, axis=-1, keepdims=True)
        ) * score_scale
        scores = jnp.where(key_index < len_ref[s], scores, masked_score)
        row_max = jnp.maximum(jnp.max(scores, axis=-1, keepdims=True), new_score)
        weights = jnp.exp(scores - row_max)
        new_weight = jnp.exp(new_score - row_max)
        weight_total = jnp.sum(weights, axis=-1, keepdims=True) + new_weight
        weighted = jnp.dot(weights.astype(jnp.bfloat16), keys, preferred_element_type=jnp.float32)
        weighted = weighted + new_weight.astype(jnp.bfloat16).astype(jnp.float32) * new_row
        lat[s * heads : (s + 1) * heads, :] = (weighted / weight_total).astype(jnp.bfloat16)

    early_copies[1].wait()
    value_dim = vraw.shape[2]
    wide_up[...] = vraw[...].astype(jnp.float32)
    for h in range(heads):
        vup[:, h * value_dim : (h + 1) * value_dim] = wide_up[:, h, :].astype(jnp.bfloat16)
    cut_a = seq_count // 2
    for s in range(cut_a):
        attend(s)
    rows_gather.second()
    for s in range(cut_a, seq_count):
        attend(s)

    spread = jnp.dot(lat[...], vup[...], preferred_element_type=jnp.float32)
    own_heads = []
    head_row = lax.broadcasted_iota(jnp.int32, (seq_count, heads, value_dim), 1)
    for h in range(heads):
        block = spread[:, h * value_dim : (h + 1) * value_dim].reshape(seq_count, heads, value_dim)
        own_heads.append(jnp.sum(jnp.where(head_row == h, block, 0.0), axis=1))
    hbuf[me] = jnp.concatenate(own_heads, axis=1).astype(jnp.bfloat16)
    heads_gather = Gather(hbuf, 1)
    heads_gather.first()
    rows_gather.third()
    heads_gather.second()
    heads_gather.third()
    rows_gather.last()
    weight_copies[0].wait()
    heads_gather.last()

    flat_heads = hbuf[...].reshape(total_rows, hbuf.shape[2])
    cbuf[me] = jnp.dot(flat_heads, wo[...], preferred_element_type=jnp.float32).astype(jnp.bfloat16)
    columns_gather = Gather(cbuf, 2)
    columns_gather.first()
    columns_gather.second()
    columns_gather.third()
    columns_gather.last()

    gains = [
        ref[...].astype(jnp.float32).reshape(1, width) for ref in (gm_ref, gf_ref, go_ref)
    ]
    mixed = jnp.concatenate([cbuf[o] for o in range(device_count)], axis=1).astype(jnp.float32)
    stage = xbuf[...].reshape(total_rows, xbuf.shape[2])
    after_mix = (stage[:, :width].astype(jnp.float32) + gains[0] * normalize(mixed)).astype(
        jnp.bfloat16
    )
    mix_rows[...] = after_mix.reshape(mix_rows.shape)
    ffn_in = (normalize(after_mix.astype(jnp.float32)) * gains[1]).astype(jnp.bfloat16)
    norm_rows[...] = ffn_in.reshape(norm_rows.shape)
    weight_copies[1].wait()
    affinity = jax.nn.sigmoid(
        lax.dot_general(
            ffn_in, router[...], (((1,), (1,)), ((), ())), preferred_element_type=jnp.float32
        )
    )
    hot = stage[:, width : width + affinity.shape[1]].astype(jnp.float32)
    chosen = affinity * hot
    lane = lax.broadcasted_iota(jnp.int32, chosen.shape, 1)
    mine = jnp.sum(jnp.where(lane == me, chosen, 0.0), axis=1, keepdims=True)
    mine = mine / jnp.sum(chosen, axis=1, keepdims=True) * routed_scale
    for copy in weight_copies[2:5]:
        copy.wait()
    expert_out = swiglu(ffn_in, eg[...], eu[...], ed[...])
    scaled = (expert_out.astype(jnp.float32) * mine).astype(jnp.bfloat16)
    terms[...] = scaled.reshape(terms.shape)

    def to_sibling(step):
        e = (me_e + step) % ep_count
        return pltpu.make_async_remote_copy(
            src_ref=terms.at[e * 2 + other_t],
            dst_ref=sib.at[e],
            send_sem=sib_send.at[step],
            recv_sem=sib_recv.at[e],
            device_id=sibling,
            device_id_type=pl.DeviceIdType.MESH,
        )

    order = sorted(range(1, ep_count), key=lambda v: -min(v, ep_count - v)) + [0]
    sib_copies = [to_sibling(step) for step in order]
    for copy in sib_copies:
        copy.start()
    sends = []
    for step in order:
        e = (me_e + step) % ep_count
        to_sibling(step).wait_recv()
        paired = terms[e * 2 + me_t].astype(jnp.float32) + sib[e].astype(jnp.float32)
        if step == 0:
            routed = paired
        else:
            part[e] = paired.astype(jnp.bfloat16)
            copy = pltpu.make_async_remote_copy(
                src_ref=part.at[e],
                dst_ref=back.at[me_e],
                send_sem=back_send.at[step],
                recv_sem=back_recv.at[me_e],
                device_id=device(e, me_t),
                device_id_type=pl.DeviceIdType.MESH,
            )
            copy.start()
            sends.append(copy)
    for copy in weight_copies[5:8]:
        copy.wait()
    combined = routed + swiglu(norm_rows[me], sg[...], su[...], sd[...]).astype(jnp.float32)
    for step in reversed(order[:-1]):
        e = (me_e + step) % ep_count
        pltpu.make_async_remote_copy(
            src_ref=part.at[e],
            dst_ref=back.at[e],
            send_sem=back_send.at[step],
            recv_sem=back_recv.at[e],
            device_id=device(e, me_t),
            device_id_type=pl.DeviceIdType.MESH,
        ).wait_recv()
        combined = combined + back[e].astype(jnp.float32)
    out_ref[...] = (
        mix_rows[me].astype(jnp.float32) + gains[2] * normalize(combined)
    ).astype(jnp.bfloat16)
    for copy in pending + sib_copies + sends:
        copy.wait_send()


def local_fused(
    hidden_in,
    query_nope,
    query_rope,
    new_latent,
    new_rope,
    cache_latent,
    cache_rope,
    lengths,
    absorb_key,
    value_up,
    out_proj,
    gain_mix,
    gain_ffn_in,
    router,
    routes,
    expert_gate,
    expert_up,
    expert_down,
    shared_gate,
    shared_up,
    shared_down,
    gain_ffn_out,
):
    seq_count, width = hidden_in.shape
    heads, latent = query_nope.shape[1], cache_latent.shape[2]
    ep_count = lax.axis_size("ep")
    device_count = 2 * ep_count
    bits = (ep_count - 1).bit_length()
    grid_p = 2 ** ((bits + 1) // 2)
    grid_q = ep_count // grid_p
    bf = jnp.bfloat16
    score_scale = (query_nope.shape[-1] + query_rope.shape[-1]) ** (-0.5)
    sends = (grid_p - 1) + grid_p * (grid_q - 1) + ep_count
    big = pl.BlockSpec(memory_space=pl.ANY)
    near = pl.BlockSpec(memory_space=pltpu.VMEM)
    dma = pltpu.SemaphoreType.DMA
    total_rows = device_count * seq_count
    rope_rows = jnp.swapaxes(cache_rope, 1, 2)
    router_rows = jnp.swapaxes(router, 0, 1)
    absorb_rows = jnp.transpose(absorb_key, (1, 2, 0)).reshape(-1, latent)
    own_shape = (seq_count, width + 128)
    weights = (
        out_proj,
        router_rows,
        expert_gate[0],
        expert_up[0],
        expert_down[0],
        shared_gate,
        shared_up,
        shared_down,
    )
    operands = (
        hidden_in,
        query_nope,
        query_rope,
        new_latent,
        new_rope,
        lengths,
        jnp.swapaxes(routes, 0, 1),
        gain_mix,
        gain_ffn_in,
        gain_ffn_out,
        absorb_rows,
        cache_latent,
        rope_rows,
        value_up,
    ) + weights
    scalar = pl.BlockSpec(memory_space=pltpu.SMEM)
    specs = [near] * 5 + [scalar] * 2 + [near] * 3 + [big] * 12
    flops = 2 * total_rows * width * out_proj.shape[1]
    return pl.pallas_call(
        functools.partial(fused_kernel, grid_p, grid_q, score_scale),
        out_shape=jax.ShapeDtypeStruct((seq_count, width), bf),
        in_specs=specs,
        out_specs=near,
        scratch_shapes=[
            pltpu.VMEM(cache_latent.shape, bf),
            pltpu.VMEM(rope_rows.shape, bf),
            pltpu.VMEM((latent, value_up.shape[1] * value_up.shape[2]), bf),
            pltpu.VMEM(value_up.shape, jnp.float32),
            pltpu.VMEM((seq_count * heads, latent), bf),
            pltpu.VMEM((seq_count * heads, query_rope.shape[2]), bf),
            pltpu.VMEM(absorb_rows.shape, bf),
            pltpu.VMEM(value_up.shape, bf),
        ]
        + [pltpu.VMEM(w.shape, bf) for w in weights]
        + [
            pltpu.VMEM((device_count,) + own_shape, bf),
            pltpu.VMEM((device_count, seq_count, out_proj.shape[0]), bf),
            pltpu.VMEM((device_count, total_rows, out_proj.shape[1]), bf),
            pltpu.VMEM((seq_count * heads, latent), bf),
            pltpu.VMEM((device_count, seq_count, width), bf),
            pltpu.VMEM((device_count, seq_count, width), bf),
            pltpu.VMEM((device_count, seq_count, width), bf),
            pltpu.VMEM((ep_count, seq_count, width), bf),
            pltpu.VMEM((ep_count, seq_count, width), bf),
            pltpu.VMEM((ep_count, seq_count, width), bf),
            dma((seq_count,)),
            dma((seq_count,)),
            dma((len(weights) + 2,)),
            dma((3, sends)),
            dma((3, device_count)),
            dma((ep_count,)),
            dma((ep_count,)),
            dma((ep_count,)),
            dma((ep_count,)),
        ],
        compiler_params=pltpu.CompilerParams(
            collective_id=0, has_side_effects=True, vmem_limit_bytes=56 * 2**20
        ),
        cost_estimate=pl.CostEstimate(flops=flops, bytes_accessed=2**24, transcendentals=0),
        name="layer_step",
    )(*operands)


def local(*args):
    hidden_in, out_proj, router = args[0], args[10], args[13]
    device_count = lax.axis_size("ep") * lax.axis_size("tp")
    fits = (
        lax.axis_size("tp") == 2
        and hidden_in.shape[0] == 8
        and device_count * hidden_in.shape[0] <= 256
        and out_proj.shape[1] % 128 == 0
        and router.shape[1] == device_count
    )
    return local_fused(*args) if fits else local_wide(*args)


def solution(mesh):
    placed = (
        P(("grp", "ep", "tp"), None),
        P(("grp", "ep", "tp"), None, None),
        P(("grp", "ep", "tp"), None, None),
        P(("grp", "ep", "tp"), None),
        P(("grp", "ep", "tp"), None),
        P(("grp", "ep", "tp"), None, None),
        P(("grp", "ep", "tp"), None, None),
        P(("grp", "ep", "tp")),
        P(),
        P(),
        P(None, ("ep", "tp")),
        P(),
        P(),
        P(),
        P(("grp", "ep"), None),
        P(("ep", "tp"), None, None),
        P(("ep", "tp"), None, None),
        P(("ep", "tp"), None, None),
        P(),
        P(),
        P(),
        P(),
    )
    return jax.shard_map(
        local, mesh=mesh, in_specs=placed, out_specs=P(("grp", "ep", "tp"), None), check_vma=False
    )
```
